32 devices in a mesh: grp: 2 (over y), fs: 4 (over z), tp: 4 (over x, core).
Axes of the slice: x: 2, y: 2, z: 4, core: 2. Of those that a mesh axis runs over, the one named last changes fastest.
Arguments:
- tokens: bfloat16 [512, 2048], P(('grp', 'fs')), parts along dimension 0, may hold values from -6 to 6
- routes: int32 [512, 2], P(('grp', 'fs')), parts along dimension 0, may hold values from 0 to 3, as said below
- route_logits: float32 [512, 2], P(('grp', 'fs')), parts along dimension 0, may hold values from -8 to 8
- gain: float32 [2048], P('fs'), may hold values from 0.1 to 1.9
- w_gate: float32 [4, 2048, 7168], P(None, 'fs', 'tp'), may hold values from -0.125 to 0.125
- w_up: float32 [4, 2048, 7168], P(None, 'fs', 'tp'), may hold values from -0.125 to 0.125
- w_down: float32 [4, 7168, 2048], P(None, 'fs', 'tp'), may hold values from -0.0625 to 0.0625
Outputs:
- gate_served: bfloat16 [8, 2048, 7168], P(('grp', 'tp'), None, 'fs'), parts along dimension 0
- up_served: bfloat16 [8, 2048, 7168], P(('grp', 'tp'), None, 'fs'), parts along dimension 0
- down_served: bfloat16 [8, 7168, 2048], P(('grp', 'tp'), 'fs'), parts along dimension 0
- mixed: bfloat16 [512, 2048], P(('grp', 'fs'), 'tp'), parts along dimension 0
The draws below stay inside these ranges and needn't reach their ends.
There are 2 independent parts, one for each index of `grp`. The reference program is written for one: setup_inputs(seed, part) draws one part's arguments, and reference() takes and returns one part's arrays. A program takes and returns all parts, laid end to end along the dimension named above; an argument that names none is the same for every part. Nothing has to cross between parts.
Inputs may be any that keep to these rules, and one draw needn't show every extreme that they name: `routes`: each row names 2 different experts; every expert is named by some row.
All inputs are finite; a program needn't handle non-finite values.
Results may differ from the reference program's by a relative error of at most 0.0085.
Values may be sent and summed in bfloat16 or wider, within the bound.
A program may use at most 192 MiB of HBM per device.

```python
import jax
import jax.numpy as jnp
from jax import lax

D = 2048
FF = 7168
EXPERTS = 4
TOP = 2
TOKENS = 256


def draw_routes(key, part):
    key_hot = jax.random.fold_in(key, 101)
    key_pick = jax.random.fold_in(key, 102)
    key_other = jax.random.fold_in(key, 103)
    key_second = jax.random.fold_in(key, 104)
    hot_expert = jax.random.randint(key_hot, (), 0, EXPERTS, dtype=jnp.int32)
    chooser = jax.random.randint(key_pick, (TOKENS,), 0, 8, dtype=jnp.int32)
    other_offset = jax.random.randint(key_other, (TOKENS,), 0, EXPERTS - 1, dtype=jnp.int32)
    other_expert = (hot_expert + 1 + other_offset) % EXPERTS
    first_col = jnp.where(chooser < 7, hot_expert, other_expert).astype(jnp.int32)
    second_offset = jax.random.randint(key_second, (TOKENS,), 0, EXPERTS - 1, dtype=jnp.int32)
    second_col = ((first_col + 1 + second_offset) % EXPERTS).astype(jnp.int32)
    row_index = jnp.arange(TOKENS, dtype=jnp.int32)
    first_col = jnp.where(row_index < EXPERTS, row_index, first_col)
    second_col = jnp.where(row_index < EXPERTS, (row_index + 1) % EXPERTS, second_col)
    return jnp.stack([first_col, second_col], axis=1).astype(jnp.int32)


def steps_of(stream_key, extent, pieces, low, largest):
    def one(axis_at, shards_of):
        draws = jax.random.uniform(jax.random.fold_in(jax.random.fold_in(stream_key, 6), axis_at), (shards_of,), jnp.float32, low / len(pieces), largest / len(pieces))
        return jnp.repeat(jnp.exp(draws), extent[axis_at] // shards_of).reshape((-1,) + (1,) * (len(extent) - axis_at - 1))

    level = one(*pieces[0])
    for cut in pieces[1:]:
        level = level * one(*cut)
    return level


def gaussian(stream_key, dims, width, reach, split=(), held_as=jnp.bfloat16):
    array = jax.random.normal(stream_key, dims, jnp.float32) * width
    if len(split) > 0:
        array = steps_of(stream_key, dims, split, -0.22, 0.18) * array
    return jnp.clip(array, min=-reach, max=reach).astype(held_as)


def setup_inputs(seed: int = 0, part: int = 0) -> dict:
    splits = jax.random.split(jax.random.key(seed), 8)
    own_keys = jax.random.split(jax.random.fold_in(splits[7], part), 8)
    tokens = gaussian(own_keys[0], (TOKENS, D), 1.0, 6.0, ((0, 4),))
    routes = draw_routes(jax.random.fold_in(jax.random.fold_in(splits[7], part), 71), part)
    route_logits = gaussian(own_keys[2], (TOKENS, TOP), 1.5, 8.0, ((0, 4),), jnp.float32)
    gain = jnp.clip(1.0 + 0.18 * jax.random.normal(splits[3], (D,), jnp.float32), 0.1, 1.9)
    w_gate = gaussian(splits[4], (EXPERTS, D, FF), D ** -0.5, 0.125, ((1, 4), (2, 4)), jnp.float32)
    w_up = gaussian(splits[5], (EXPERTS, D, FF), D ** -0.5, 0.125, ((1, 4), (2, 4)), jnp.float32)
    w_down = gaussian(splits[6], (EXPERTS, FF, D), FF ** -0.5, 0.0625, ((1, 4), (2, 4)), jnp.float32)
    return {"tokens": tokens, "routes": routes, "route_logits": route_logits, "gain": gain, "w_gate": w_gate, "w_up": w_up, "w_down": w_down}


def reference(tokens, routes, route_logits, gain, w_gate, w_up, w_down):
    values = tokens.astype(jnp.float32)
    mean_square = lax.optimization_barrier(jnp.mean(values * values, axis=-1, keepdims=True))
    normed = (values * lax.rsqrt(mean_square + 1e-06)).astype(jnp.bfloat16)
    first = jax.nn.sigmoid(route_logits[:, 0] - route_logits[:, 1])
    second = jax.nn.sigmoid(route_logits[:, 1] - route_logits[:, 0])
    gate_cast = (w_gate * gain[None, :, None]).astype(jnp.bfloat16)
    up_cast = (w_up * gain[None, :, None]).astype(jnp.bfloat16)
    down_cast = w_down.astype(jnp.bfloat16)
    total = jnp.zeros((tokens.shape[0], w_down.shape[2]), jnp.float32)
    for expert in range(EXPERTS):
        weight_col = first * (routes[:, 0] == expert).astype(jnp.float32)
        weight_col = weight_col + second * (routes[:, 1] == expert).astype(jnp.float32)
        weight_col = weight_col.astype(jnp.bfloat16)
        gate_act = jnp.dot(normed, gate_cast[expert], preferred_element_type=jnp.float32)
        up_act = jnp.dot(normed, up_cast[expert], preferred_element_type=jnp.float32)
        hidden = (jax.nn.silu(gate_act) * up_act * weight_col[:, None].astype(jnp.float32)).astype(jnp.bfloat16)
        total = total + jnp.dot(hidden, down_cast[expert], preferred_element_type=jnp.float32)
    return (gate_cast, up_cast, down_cast, total.astype(jnp.bfloat16))
```

```python
import functools

import jax
import jax.numpy as jnp
from jax import lax
from jax.experimental import pallas as pl
from jax.experimental.pallas import tpu as pltpu
from jax.sharding import PartitionSpec as P

BF16 = jnp.bfloat16
F32 = jnp.float32
CHUNKS = 4
DOWN_CHUNKS = 4
LOADS = 3
DOWN_LOADS = 2
STEPS = 18
OUTER_LEAD = 2
OUTER_OWN = (0, 0, 1, 1, 2, 2, 3, 4, 6)
OUTER_RELAY = (1, 1, 2, 2, 3, 3, 4, 5, 8)
NEAR_LAG = 1
IN_RATE, IN_LAG = 0.6, 1.0
OUT_RATE, OUT_LAG = 0.5, 0.8
LANES = 128


def move_kernel(
    groups, n, tokens_ref, routes_ref, logits_ref, gain_ref, wg_ref, wu_ref, wd_ref, x_ref, gu_ref, od_ref,
    wide, wide_d, stage, extra, relay, stage_d, tok, pack, route_v, logit_v, gain_v, gain_col,
    load_sem, load_d_sem, small_sem, s1s, s1r, xs, xr, zs, zr, ys, yr, ds, dr, ts, tr, os, ov, ms, mr, own_sem,
):
    g, f, t = lax.axis_index("grp"), lax.axis_index("fs"), lax.axis_index("tp")
    rows = wg_ref.shape[1]
    half = rows // groups
    ch = half // CHUNKS
    hidden, width = wd_ref.shape[1:]
    dh = hidden // DOWN_CHUNKS
    items = 2 * CHUNKS
    count, depth = tokens_ref.shape
    part = count // n
    weights = (wg_ref, wu_ref)

    core = lax.rem(t, 2)
    mate = t + 1 - 2 * core
    peers = (t, mate, lax.rem(t + 2, n), lax.rem(mate + 2, n))
    home = f == t
    order = (2, 3, 0, 1)
    near = f + 1 - 2 * lax.rem(f, 2)
    low = f < n // 2
    far = (jnp.where(low, 2, 1), jnp.where(low, 3, 0))

    def remote(src, dst, ssem, rsem, where):
        return pltpu.make_async_remote_copy(
            src_ref=src, dst_ref=dst, send_sem=ssem, recv_sem=rsem,
            device_id=where, device_id_type=pl.DeviceIdType.MESH,
        )

    def own_row(c):
        return pl.multiple_of(g * half + c * ch, ch)

    def other_row(c):
        return pl.multiple_of((1 - g) * half + c * ch, ch)

    def load(i, k, row):
        slot = i % LOADS
        src = weights[i // CHUNKS].at[peers[k], pl.ds(row(i % CHUNKS), ch), :]
        return pltpu.make_async_copy(src, wide.at[slot, k], load_sem.at[slot, k])

    for i in range(LOADS):
        for k in order:
            load(i, k, own_row).start()
    small = (
        pltpu.make_async_copy(gain_ref, gain_v, small_sem.at[0]),
        pltpu.make_async_copy(tokens_ref, tok, small_sem.at[1]),
        pltpu.make_async_copy(routes_ref, route_v, small_sem.at[2]),
        pltpu.make_async_copy(logits_ref, logit_v, small_sem.at[3]),
    )
    for copy in small:
        copy.start()

    barrier = pltpu.get_barrier_semaphore()

    def greet(where):
        pl.semaphore_signal(barrier, inc=1, device_id=where, device_id_type=pl.DeviceIdType.MESH)

    for k in (1, 2, 3):
        greet((g, f, peers[k]))
    for d in range(1, n):
        for k in (0, 1):
            greet((g, lax.rem(f + d, n), peers[k]))
    greet((1 - g, f, t))

    small[0].wait()
    for b in range(rows // LANES):
        line = gain_v[0:1, b * LANES : (b + 1) * LANES]
        eye = lax.broadcasted_iota(jnp.int32, (LANES, LANES), 0) == lax.broadcasted_iota(jnp.int32, (LANES, LANES), 1)
        column = jnp.sum(jnp.where(eye, jnp.broadcast_to(line, (LANES, LANES)), 0.0), axis=1, keepdims=True)
        gain_col[b * LANES : (b + 1) * LANES, :] = jnp.broadcast_to(column, (LANES, LANES))
    pl.semaphore_wait(barrier, 2 * n + 2)

    def at_rows(i, source, row):
        start = i // CHUNKS * (rows * n) + source * rows + row
        return gu_ref.at[pl.ds(pl.multiple_of(start, ch), ch), :]

    def own_piece(i, source):
        return at_rows(i, source, own_row(i % CHUNKS))

    def other_piece(i, source):
        return at_rows(i, source, other_row(i % CHUNKS))

    def first(k, i):
        return remote(stage.at[k, i], relay.at[k - 2, i], s1s.at[k, i], s1r.at[k, i], (g, f, peers[k]))

    def first_home(k, i):
        return remote(stage.at[k, i], own_piece(i, f), s1s.at[k, i], s1r.at[k, i], (g, f, peers[k]))

    def own_home(i):
        return pltpu.make_async_copy(stage.at[0, i], own_piece(i, f), s1s.at[0, i])

    def direct(k, i):
        return remote(stage.at[k, i], own_piece(i, f), zs.at[k, i], zr.at[f, i], (g, t, peers[k]))

    def layer(k, i):
        return remote(relay.at[k - 2, i], own_piece(i, f), zs.at[k, i], zr.at[f, i], (g, peers[k], t))

    def layer_in(source, i):
        piece = own_piece(i, source)
        return remote(piece, piece, zs.at[0, i], zr.at[source, i], (1 - g, f, t))

    def across(source, i):
        piece = own_piece(i, source)
        return remote(piece, piece, ys.at[source, i], yr.at[source, i], (1 - g, f, t))

    def extra_home(i):
        return pltpu.make_async_copy(extra.at[0, i], other_piece(i, f), xs.at[0, i])

    def extra_mate(i):
        return remote(extra.at[1, i], other_piece(i, f), xs.at[1, i], xr.at[i], (g, f, mate))

    def down(k, c):
        src = stage_d.at[k, c]
        dst = od_ref.at[pl.ds(c * dh, dh), pl.ds(pl.multiple_of(t * width, LANES), width)]
        if k == 0:
            return pltpu.make_async_copy(src, dst, ds.at[0, c])
        return remote(src, dst, ds.at[k, c], dr.at[k, c], (g, f, peers[k]))

    def load_d(k, c):
        slot = c % DOWN_LOADS
        return pltpu.make_async_copy(wd_ref.at[peers[k], pl.ds(c * dh, dh), :], wide_d.at[slot, k], load_d_sem.at[slot, k])

    def fold(slot, k, row, dst):
        scale = gain_col[pl.ds(row, ch), 0:1]
        dst[...] = (wide[slot, k] * scale).astype(BF16)

    def piece(source, q):
        return x_ref.at[pl.ds(pl.multiple_of(source * count + q * part, part), part), :]

    def token_out(d):
        src = pack.at[pl.ds(pl.multiple_of(t * part, part), part), :]
        return remote(src, piece(f, t), ts.at[d], tr.at[f], (g, lax.rem(f + d, n), t))

    def token_in(source):
        return remote(piece(source, t), piece(source, t), ts.at[0], tr.at[source], (g, f, t))

    def token_over(source):
        here = piece(source, t)
        return remote(here, here, os.at[source], ov.at[source], (g, f, peers[2]))

    def token_from_over(source):
        here = piece(source, peers[2])
        return remote(here, here, os.at[source], ov.at[source], (g, f, peers[2]))

    def token_mate(source, j):
        here = piece(source, (t, peers[2])[j])
        return remote(here, here, ms.at[j, source], mr.at[j, source], (g, f, mate))

    def token_from_mate(source, j):
        here = piece(source, (mate, peers[3])[j])
        return remote(here, here, ms.at[j, source], mr.at[j, source], (g, f, mate))

    def token_own():
        return pltpu.make_async_copy(pack, x_ref.at[pl.ds(pl.multiple_of(f * count, count), count), :], own_sem.at[0])

    def send_tokens():
        for copy in small[1:]:
            copy.wait()
        values = tok[...].astype(F32)
        mean_square = jnp.mean(values * values, axis=-1, keepdims=True)
        pack[:, :depth] = (values * lax.rsqrt(mean_square + 1e-06)).astype(BF16)
        diff = logit_v[0:1, :] - logit_v[1:2, :]
        first_w = 1.0 / (1.0 + jnp.exp(-diff))
        second_w = 1.0 / (1.0 + jnp.exp(diff))
        eye = lax.broadcasted_iota(jnp.int32, (count, count), 0) == lax.broadcasted_iota(jnp.int32, (count, count), 1)
        lane = lax.broadcasted_iota(jnp.int32, (count, LANES), 1)
        table = jnp.zeros((count, LANES), F32)
        for e in range(n):
            line = first_w * (route_v[0:1, :] == e).astype(F32) + second_w * (route_v[1:2, :] == e).astype(F32)
            column = jnp.sum(jnp.where(eye, jnp.broadcast_to(line, (count, count)), 0.0), axis=1, keepdims=True)
            table = jnp.where(lane == e, jnp.broadcast_to(column, (count, LANES)), table)
        pack[:, depth:] = table.astype(BF16)
        token_own().start()
        for d in range(1, n):
            token_out(d).start()

    def share_tokens():
        for d in range(1, n):
            source = lax.rem(f + d, n)
            token_in(source).wait_recv()
            token_over(source).start()
            token_mate(source, 0).start()

    def pair_tokens():
        for d in range(1, n):
            source = lax.rem(f + d, n)
            token_from_over(source).wait_recv()
            token_mate(source, 1).start()

    def produce(i):
        for k in order:
            load(i, k, own_row).wait()
            fold(i % LOADS, k, own_row(i % CHUNKS), stage.at[k, i])
            if i + LOADS < items:
                load(i + LOADS, k, own_row).start()

            @pl.when(home)
            def _():
                if k == 0:
                    own_home(i).start()
                else:
                    first_home(k, i).start()

            if k >= 2:
                @pl.when(jnp.logical_not(home))
                def _():
                    first(k, i).start()

    def own(i, where):
        @pl.when(where)
        def _():
            direct(0, i).start()
            direct(1, i).start()

    def relay_home(i):
        for k in (2, 3):
            @pl.when(peers[k] == f)
            def _():
                first_home(k, i).wait_recv()
                across(f, i).start()

    def relay_near(i):
        for k in (2, 3):
            @pl.when(peers[k] == near)
            def _():
                first(k, i).wait_recv()
                layer(k, i).start()

    def relay_far(i, where):
        for k in (2, 3):
            @pl.when(where & (peers[k] != f) & (peers[k] != near))
            def _():
                first(k, i).wait_recv()
                layer(k, i).start()

    def turn(source, i):
        layer_in(source, i).wait_recv()
        across(source, i).start()

    def down_step(c):
        for k in order:
            load_d(k, c).wait()
            stage_d[k, c] = wide_d[c % DOWN_LOADS, k].astype(BF16)
            if c + DOWN_LOADS < DOWN_CHUNKS:
                load_d(k, c + DOWN_LOADS).start()
            down(k, c).start()

    def home_step(i):
        for k in (0, 1):
            load(i, k, other_row).wait()
            fold(i % LOADS, k, other_row(i % CHUNKS), extra.at[k, i])
            if i + LOADS < items:
                load(i + LOADS, k, other_row).start()
            (extra_home if k == 0 else extra_mate)(i).start()

    outer = (f == 0) | (f == n - 1)
    inner = jnp.logical_not(outer)
    own_far = (t != near) & jnp.logical_not(home)
    send_tokens()
    for i in range(items):
        produce(i)
        own(i, t == near)
        own(i, own_far & inner)
        if i < OUTER_LEAD:
            own(i, own_far & outer)
        if i == 1:
            for c in range(DOWN_LOADS):
                for k in order:
                    load_d(k, c).start()
    sent = {"own": OUTER_LEAD, "relay": 0, "near": 0, "in": 0, "out": 0}

    def up_to(name, limit, act):
        while sent[name] < min(limit, items):
            act(sent[name])
            sent[name] += 1

    for s in range(STEPS):
        if s < items:
            relay_home(s)
            relay_near(s)
            relay_far(s, inner)
        up_to("own", OUTER_LEAD + OUTER_OWN[min(s, len(OUTER_OWN) - 1)], lambda i: own(i, own_far & outer))
        up_to("relay", OUTER_RELAY[min(s, len(OUTER_RELAY) - 1)], lambda i: relay_far(i, outer))
        if s == 0:
            share_tokens()
        if 1 <= s <= DOWN_CHUNKS:
            down_step(s - 1)
        if s == items + 1:
            pair_tokens()
        up_to("near", s + 1 - NEAR_LAG, lambda i: turn(near, i))
        up_to("in", int((s + 1) * IN_RATE - IN_LAG), lambda i: turn(far[0], i))
        up_to("out", int((s + 1) * OUT_RATE - OUT_LAG), lambda i: turn(far[1], i))
        if s == items:
            @pl.when(home)
            def _():
                for j in range(LOADS):
                    for k in (0, 1):
                        load(j, k, other_row).start()
                for j in range(items):
                    home_step(j)
    assert min(sent.values()) == items

    def finish(i, _):
        @pl.when(home)
        def _():
            own_home(i).wait()
            extra_home(i).wait()
            extra_mate(i).wait_send()
            first_home(1, i).wait_send()

        @pl.when(jnp.logical_not(home))
        def _():
            direct(0, i).wait_send()
            direct(1, i).wait_send()

        @pl.when(f == mate)
        def _():
            first_home(1, i).wait_recv()
            extra_mate(i).wait_recv()

        for k in (2, 3):
            first(k, i).wait_send()

            @pl.when(peers[k] != f)
            def _():
                layer(k, i).wait_send()

            @pl.when(peers[k] == f)
            def _():
                across(f, i).wait()

        for source in (near, *far):
            across(source, i).wait()
        return 0

    lax.fori_loop(0, items, finish, 0)

    def finish_d(c, _):
        for k in range(n):
            down(k, c).wait()
        return 0

    lax.fori_loop(0, DOWN_CHUNKS, finish_d, 0)
    token_own().wait()
    for d in range(1, n):
        source = lax.rem(f + d, n)
        token_out(d).wait_send()
        token_over(source).wait_send()
        for j in range(2):
            token_mate(source, j).wait_send()
            token_from_mate(source, j).wait_recv()


def move(groups, n, tokens, routes, route_logits, gain, w_gate, w_up, w_down):
    experts, rows, cols = w_gate.shape
    hidden, width = w_down.shape[1:]
    count, depth = tokens.shape
    ch = rows // groups // CHUNKS
    dh = hidden // DOWN_CHUNKS
    items = 2 * CHUNKS
    dma = pltpu.SemaphoreType.DMA
    hbm = pl.BlockSpec(memory_space=pl.ANY)
    return pl.pallas_call(
        functools.partial(move_kernel, groups, n),
        out_shape=(
            jax.ShapeDtypeStruct((count * n, depth + LANES), BF16),
            jax.ShapeDtypeStruct((2 * rows * n, cols), BF16),
            jax.ShapeDtypeStruct((hidden, width * n), BF16),
        ),
        in_specs=[hbm] * 7,
        out_specs=(hbm, hbm, hbm),
        scratch_shapes=[
            pltpu.VMEM((LOADS, n, ch, cols), F32),
            pltpu.VMEM((DOWN_LOADS, n, dh, width), F32),
            pltpu.VMEM((n, items, ch, cols), BF16),
            pltpu.VMEM((2, items, ch, cols), BF16),
            pltpu.VMEM((2, items, ch, cols), BF16),
            pltpu.VMEM((n, DOWN_CHUNKS, dh, width), BF16),
            pltpu.VMEM((count, depth), BF16),
            pltpu.VMEM((count, depth + LANES), BF16),
            pltpu.VMEM((2, count), jnp.int32),
            pltpu.VMEM((2, count), F32),
            pltpu.VMEM((1, rows), F32),
            pltpu.VMEM((rows, LANES), F32),
            dma((LOADS, n)),
            dma((DOWN_LOADS, n)),
            dma((4,)),
            dma((n, items)),
            dma((n, items)),
            dma((2, items)),
            dma((items,)),
            dma((n, items)),
            dma((n, items)),
            dma((n, items)),
            dma((n, items)),
            dma((n, DOWN_CHUNKS)),
            dma((n, DOWN_CHUNKS)),
            dma((n,)),
            dma((n,)),
            dma((n,)),
            dma((n,)),
            dma((2, n)),
            dma((2, n)),
            dma((1,)),
        ],
        name="move_weights",
        compiler_params=pltpu.CompilerParams(
            collective_id=0, has_side_effects=True, vmem_limit_bytes=56 << 20
        ),
    )(tokens, routes.T, route_logits.T, gain.reshape(1, rows), w_gate, w_up, w_down)


def mix_kernel(rows_ref, weight_ref, gate_ref, up_ref, down_ref, gate_out, up_out, down_out, term_ref, total):
    j = pl.program_id(0)

    @pl.when(j == 0)
    def _():
        total[...] = jnp.zeros_like(total)

    gate, up, down = gate_ref[...], up_ref[...], down_ref[...]
    gate_out[...], up_out[...], down_out[...] = gate, up, down
    x = rows_ref[...]
    gate_act = jnp.dot(x, gate, preferred_element_type=F32)
    up_act = jnp.dot(x, up, preferred_element_type=F32)
    lane = lax.broadcasted_iota(jnp.int32, weight_ref.shape, 1)
    table = jnp.where(lane == lax.axis_index("tp"), weight_ref[...].astype(F32), 0.0)
    scale = jnp.sum(table, axis=1, keepdims=True)
    hidden = (gate_act / (1.0 + jnp.exp(-gate_act)) * up_act * scale).astype(BF16)
    total[...] += jnp.dot(hidden, down, preferred_element_type=F32)

    @pl.when(j == pl.num_programs(0) - 1)
    def _():
        term_ref[...] = total[...].astype(BF16)


def mix(packed, both, down):
    count, depth = packed.shape[0], packed.shape[1] - LANES
    cols = both.shape[1]
    wide = down.shape[1]
    tile = next(w for w in (256, 128) if cols % w == 0)
    whole = pl.BlockSpec((count, depth), lambda j: (0, 0))
    column = pl.BlockSpec((depth, tile), lambda j: (0, j))
    second = pl.BlockSpec((depth, tile), lambda j: (1, j))
    row = pl.BlockSpec((tile, wide), lambda j: (j, 0))
    return pl.pallas_call(
        mix_kernel,
        grid=(cols // tile,),
        out_shape=(
            jax.ShapeDtypeStruct((depth, cols), BF16),
            jax.ShapeDtypeStruct((depth, cols), BF16),
            jax.ShapeDtypeStruct(down.shape, BF16),
            jax.ShapeDtypeStruct((count, wide), BF16),
        ),
        in_specs=[whole, pl.BlockSpec((count, LANES), lambda j: (0, depth // LANES)), column, second, row],
        out_specs=(column, column, row, pl.BlockSpec((count, wide), lambda j: (0, 0))),
        scratch_shapes=[pltpu.VMEM((count, wide), F32)],
        name="mix_tokens",
        compiler_params=pltpu.CompilerParams(vmem_limit_bytes=48 << 20),
    )(packed, packed, both, both, down)


def sum_kernel(n, term_ref, out_ref, near, near_in, far, far_in, last, last_in, s1, r1, s2, r2, s3, r3):
    g, f, t = lax.axis_index("grp"), lax.axis_index("fs"), lax.axis_index("tp")
    mesh_id = pl.DeviceIdType.MESH
    width = out_ref.shape[1]
    count = out_ref.shape[0]
    mate = t + 1 - 2 * lax.rem(t, 2)
    over = lax.rem(t + 2, n)
    mate_over = lax.rem(mate + 2, n)

    barrier = pltpu.get_barrier_semaphore()
    for e in (mate, over):
        pl.semaphore_signal(barrier, inc=1, device_id=(g, f, e), device_id_type=mesh_id)
    for d in range(1, n):
        pl.semaphore_signal(barrier, inc=1, device_id=(g, lax.rem(f + d, n), t), device_id_type=mesh_id)
    pl.semaphore_wait(barrier, n + 1)

    def block(layer, column):
        return term_ref.at[pl.ds(pl.multiple_of(layer * count, count), count), pl.ds(pl.multiple_of(column * width, width), width)]

    def remote(src, dst, ssem, rsem, where):
        return pltpu.make_async_remote_copy(
            src_ref=src, dst_ref=dst, send_sem=ssem, recv_sem=rsem, device_id=where, device_id_type=mesh_id
        )

    layers = [lax.rem(f + d, n) for d in (2, 1, 3, 0)]

    def to_mate(i, h):
        column = mate_over if h == 0 else mate
        return remote(block(layers[i], column), near_in.at[h, i], s1.at[h, i], r1.at[h, i], (g, f, mate))

    def to_over(i):
        return remote(far.at[i], far_in.at[i], s2.at[i], r2.at[i], (g, f, over))

    def to_layer(i):
        return remote(last.at[i], last_in.at[f], s3.at[i], r3.at[f], (g, layers[i], t))

    def from_layer(layer):
        return remote(last.at[0], last_in.at[layer], s3.at[0], r3.at[layer], (g, layer, t))

    for i in range(n):
        for h in range(2):
            to_mate(i, h).start()
    for i in range(n):
        to_mate(i, 0).wait_recv()
        far[i] = (block(layers[i], over)[...].astype(F32) + near_in[0, i].astype(F32)).astype(BF16)
        to_mate(i, 1).wait_recv()
        near[i] = block(layers[i], t)[...].astype(F32) + near_in[1, i].astype(F32)
        to_over(i).start()
    for i in range(n):
        to_over(i).wait_recv()
        near[i] = near[i] + far_in[i].astype(F32)
        if i < n - 1:
            last[i] = near[i].astype(BF16)
            to_layer(i).start()
    total = near[n - 1]
    for d in range(1, n):
        layer = lax.rem(f + d, n)
        from_layer(layer).wait_recv()
        total = total + last_in[layer].astype(F32)
    out_ref[...] = total.astype(BF16)
    for i in range(n):
        for h in range(2):
            to_mate(i, h).wait_send()
        to_over(i).wait_send()
        if i < n - 1:
            to_layer(i).wait_send()


def sum_terms(n, term):
    count, width = term.shape[0] // n, term.shape[1] // n
    dma = pltpu.SemaphoreType.DMA
    vmem = pl.BlockSpec(memory_space=pltpu.VMEM)
    piece = (count, width)
    return pl.pallas_call(
        functools.partial(sum_kernel, n),
        out_shape=jax.ShapeDtypeStruct(piece, BF16),
        in_specs=[vmem],
        out_specs=vmem,
        scratch_shapes=[
            pltpu.VMEM((n, *piece), F32),
            pltpu.VMEM((2, n, *piece), BF16),
            pltpu.VMEM((n, *piece), BF16),
            pltpu.VMEM((n, *piece), BF16),
            pltpu.VMEM((n, *piece), BF16),
            pltpu.VMEM((n, *piece), BF16),
            dma((2, n)), dma((2, n)), dma((n,)), dma((n,)), dma((n,)), dma((n,)),
        ],
        name="sum_terms",
        compiler_params=pltpu.CompilerParams(collective_id=1, has_side_effects=True),
    )(term)


def fits(mesh, tokens, w_gate, w_down):
    groups, n, tp = mesh.shape["grp"], mesh.shape["fs"], mesh.shape["tp"]
    rows, cols = w_gate.shape[1:]
    hidden, width = w_down.shape[1:]
    return (
        groups == 2 and n == 4 and tp == 4 and w_gate.shape[0] == tp
        and cols == hidden and cols % 128 == 0 and width % 128 == 0 and tokens.shape[0] % (16 * n) == 0
        and rows % (groups * CHUNKS * 16) == 0 and hidden % (DOWN_CHUNKS * 16) == 0
        and tokens.shape[0] * n <= 512 and rows % LANES == 0 and rows * n == tokens.shape[1]
    )


def body(mesh, tokens, routes, route_logits, gain, w_gate, w_up, w_down):
    n, depth = mesh.shape["fs"], tokens.shape[1]
    if fits(mesh, tokens, w_gate, w_down):
        packed, both, down = move(mesh.shape["grp"], n, tokens, routes, route_logits, gain, w_gate, w_up, w_down)
        gate, up, down, term = mix(packed, both, down)
        return gate[None], up[None], down[None], sum_terms(n, term)
    values = tokens.astype(F32)
    mean_square = jnp.mean(values * values, axis=-1, keepdims=True)
    normed = (values * lax.rsqrt(mean_square + 1e-06)).astype(BF16)
    expert_id = lax.axis_index("tp")
    first = jax.nn.sigmoid(route_logits[:, 0] - route_logits[:, 1])
    second = jax.nn.sigmoid(route_logits[:, 1] - route_logits[:, 0])
    weight_col = first * (routes[:, 0] == expert_id).astype(F32)
    weight_col = (weight_col + second * (routes[:, 1] == expert_id).astype(F32)).astype(BF16)
    packed = jnp.concatenate([normed, jnp.broadcast_to(weight_col[:, None], (normed.shape[0], 128))], axis=1)
    packed = lax.all_gather(packed, "fs", axis=0, tiled=True)
    gate = (w_gate * gain[None, :, None]).astype(BF16)
    up = (w_up * gain[None, :, None]).astype(BF16)
    spread = functools.partial(lax.all_to_all, axis_name="tp", split_axis=0, concat_axis=2, tiled=True)
    gate, up, down = spread(gate), spread(up), spread(w_down.astype(BF16))
    stack = functools.partial(lax.all_to_all, axis_name="fs", split_axis=2, concat_axis=1, tiled=True)
    gate, up = stack(gate), stack(up)
    rows, weight = packed[:, :depth], packed[:, depth : depth + 1]
    gate_act = jnp.dot(rows, gate[0], preferred_element_type=F32)
    up_act = jnp.dot(rows, up[0], preferred_element_type=F32)
    hidden = (jax.nn.silu(gate_act) * up_act * weight.astype(F32)).astype(BF16)
    term = jnp.dot(hidden, down[0], preferred_element_type=F32)
    by_feature = lax.psum_scatter(term, "tp", scatter_dimension=1, tiled=True)
    mixed = lax.psum_scatter(by_feature, "fs", scatter_dimension=0, tiled=True)
    return gate, up, down, mixed.astype(BF16)


def solution(mesh):
    return jax.shard_map(
        functools.partial(body, mesh),
        mesh=mesh,
        in_specs=(
            P(("grp", "fs"), None),
            P(("grp", "fs"), None),
            P(("grp", "fs"), None),
            P("fs"),
            P(None, "fs", "tp"),
            P(None, "fs", "tp"),
            P(None, "fs", "tp"),
        ),
        out_specs=(
            P(("grp", "tp"), None, "fs"),
            P(("grp", "tp"), None, "fs"),
            P(("grp", "tp"), "fs", None),
            P(("grp", "fs"), "tp"),
        ),
        check_vma=False,
    )
```

```python
import functools

import jax
import jax.numpy as jnp
from jax import lax
from jax.experimental import pallas as pl
from jax.experimental.pallas import tpu as pltpu
from jax.sharding import PartitionSpec as P

BF16 = jnp.bfloat16
F32 = jnp.float32
CHUNKS = 4
DOWN_CHUNKS = 4
LOADS = 3
DOWN_LOADS = 2
STEPS = 18
OUTER_LEAD = 2
OUTER_OWN = (0, 0, 1, 1, 2, 2, 3, 4, 6)
OUTER_RELAY = (1, 1, 2, 2, 3, 3, 4, 5, 8)
NEAR_LAG = 1
IN_RATE, IN_LAG = 0.6, 1.0
OUT_RATE, OUT_LAG = 0.5, 0.8
LANES = 128


def move_kernel(
    groups, n, tokens_ref, routes_ref, logits_ref, gain_ref, wg_ref, wu_ref, wd_ref, x_ref, og_ref, ou_ref, od_ref,
    wide, wide_d, stage, extra, relay, stage_d, tok, pack, route_v, logit_v, gain_v, gain_col,
    load_sem, load_d_sem, small_sem, s1s, s1r, xs, xr, zs, zr, ys, yr, ds, dr, ts, tr, os, ov, ms, mr, own_sem,
):
    g, f, t = lax.axis_index("grp"), lax.axis_index("fs"), lax.axis_index("tp")
    rows = wg_ref.shape[1]
    half = rows // groups
    ch = half // CHUNKS
    hidden, width = wd_ref.shape[1:]
    dh = hidden // DOWN_CHUNKS
    items = 2 * CHUNKS
    count, depth = tokens_ref.shape
    part = count // n
    weights = (wg_ref, wu_ref)

    core = lax.rem(t, 2)
    mate = t + 1 - 2 * core
    peers = (t, mate, lax.rem(t + 2, n), lax.rem(mate + 2, n))
    home = f == t
    order = (2, 3, 0, 1)
    near = f + 1 - 2 * lax.rem(f, 2)
    low = f < n // 2
    far = (jnp.where(low, 2, 1), jnp.where(low, 3, 0))

    def remote(src, dst, ssem, rsem, where):
        return pltpu.make_async_remote_copy(
            src_ref=src, dst_ref=dst, send_sem=ssem, recv_sem=rsem,
            device_id=where, device_id_type=pl.DeviceIdType.MESH,
        )

    def own_row(c):
        return pl.multiple_of(g * half + c * ch, ch)

    def other_row(c):
        return pl.multiple_of((1 - g) * half + c * ch, ch)

    def load(i, k, row):
        slot = i % LOADS
        src = weights[i // CHUNKS].at[peers[k], pl.ds(row(i % CHUNKS), ch), :]
        return pltpu.make_async_copy(src, wide.at[slot, k], load_sem.at[slot, k])

    for i in range(LOADS):
        for k in order:
            load(i, k, own_row).start()
    small = (
        pltpu.make_async_copy(gain_ref, gain_v, small_sem.at[0]),
        pltpu.make_async_copy(tokens_ref, tok, small_sem.at[1]),
        pltpu.make_async_copy(routes_ref, route_v, small_sem.at[2]),
        pltpu.make_async_copy(logits_ref, logit_v, small_sem.at[3]),
    )
    for copy in small:
        copy.start()

    barrier = pltpu.get_barrier_semaphore()

    def greet(where):
        pl.semaphore_signal(barrier, inc=1, device_id=where, device_id_type=pl.DeviceIdType.MESH)

    for k in (1, 2, 3):
        greet((g, f, peers[k]))
    for d in range(1, n):
        for k in (0, 1):
            greet((g, lax.rem(f + d, n), peers[k]))
    greet((1 - g, f, t))

    small[0].wait()
    for b in range(rows // LANES):
        line = gain_v[0:1, b * LANES : (b + 1) * LANES]
        eye = lax.broadcasted_iota(jnp.int32, (LANES, LANES), 0) == lax.broadcasted_iota(jnp.int32, (LANES, LANES), 1)
        column = jnp.sum(jnp.where(eye, jnp.broadcast_to(line, (LANES, LANES)), 0.0), axis=1, keepdims=True)
        gain_col[b * LANES : (b + 1) * LANES, :] = jnp.broadcast_to(column, (LANES, LANES))
    pl.semaphore_wait(barrier, 2 * n + 2)

    def at_rows(i, source, row):
        return (og_ref, ou_ref)[i // CHUNKS].at[pl.ds(pl.multiple_of(source * rows + row, ch), ch), :]

    def own_piece(i, source):
        return at_rows(i, source, own_row(i % CHUNKS))

    def other_piece(i, source):
        return at_rows(i, source, other_row(i % CHUNKS))

    def first(k, i):
        return remote(stage.at[k, i], relay.at[k - 2, i], s1s.at[k, i], s1r.at[k, i], (g, f, peers[k]))

    def first_home(k, i):
        return remote(stage.at[k, i], own_piece(i, f), s1s.at[k, i], s1r.at[k, i], (g, f, peers[k]))

    def own_home(i):
        return pltpu.make_async_copy(stage.at[0, i], own_piece(i, f), s1s.at[0, i])

    def direct(k, i):
        return remote(stage.at[k, i], own_piece(i, f), zs.at[k, i], zr.at[f, i], (g, t, peers[k]))

    def layer(k, i):
        return remote(relay.at[k - 2, i], own_piece(i, f), zs.at[k, i], zr.at[f, i], (g, peers[k], t))

    def layer_in(source, i):
        piece = own_piece(i, source)
        return remote(piece, piece, zs.at[0, i], zr.at[source, i], (1 - g, f, t))

    def across(source, i):
        piece = own_piece(i, source)
        return remote(piece, piece, ys.at[source, i], yr.at[source, i], (1 - g, f, t))

    def extra_home(i):
        return pltpu.make_async_copy(extra.at[0, i], other_piece(i, f), xs.at[0, i])

    def extra_mate(i):
        return remote(extra.at[1, i], other_piece(i, f), xs.at[1, i], xr.at[i], (g, f, mate))

    def down(k, c):
        src = stage_d.at[k, c]
        dst = od_ref.at[pl.ds(c * dh, dh), pl.ds(pl.multiple_of(t * width, LANES), width)]
        if k == 0:
            return pltpu.make_async_copy(src, dst, ds.at[0, c])
        return remote(src, dst, ds.at[k, c], dr.at[k, c], (g, f, peers[k]))

    def load_d(k, c):
        slot = c % DOWN_LOADS
        return pltpu.make_async_copy(wd_ref.at[peers[k], pl.ds(c * dh, dh), :], wide_d.at[slot, k], load_d_sem.at[slot, k])

    def fold(slot, k, row, dst):
        scale = gain_col[pl.ds(row, ch), 0:1]
        dst[...] = (wide[slot, k] * scale).astype(BF16)

    def piece(source, q):
        return x_ref.at[pl.ds(pl.multiple_of(source * count + q * part, part), part), :]

    def token_out(d):
        src = pack.at[pl.ds(pl.multiple_of(t * part, part), part), :]
        return remote(src, piece(f, t), ts.at[d], tr.at[f], (g, lax.rem(f + d, n), t))

    def token_in(source):
        return remote(piece(source, t), piece(source, t), ts.at[0], tr.at[source], (g, f, t))

    def token_over(source):
        here = piece(source, t)
        return remote(here, here, os.at[source], ov.at[source], (g, f, peers[2]))

    def token_from_over(source):
        here = piece(source, peers[2])
        return remote(here, here, os.at[source], ov.at[source], (g, f, peers[2]))

    def token_mate(source, j):
        here = piece(source, (t, peers[2])[j])
        return remote(here, here, ms.at[j, source], mr.at[j, source], (g, f, mate))

    def token_from_mate(source, j):
        here = piece(source, (mate, peers[3])[j])
        return remote(here, here, ms.at[j, source], mr.at[j, source], (g, f, mate))

    def token_own():
        return pltpu.make_async_copy(pack, x_ref.at[pl.ds(pl.multiple_of(f * count, count), count), :], own_sem.at[0])

    def send_tokens():
        for copy in small[1:]:
            copy.wait()
        values = tok[...].astype(F32)
        mean_square = jnp.mean(values * values, axis=-1, keepdims=True)
        pack[:, :depth] = (values * lax.rsqrt(mean_square + 1e-06)).astype(BF16)
        diff = logit_v[0:1, :] - logit_v[1:2, :]
        first_w = 1.0 / (1.0 + jnp.exp(-diff))
        second_w = 1.0 / (1.0 + jnp.exp(diff))
        eye = lax.broadcasted_iota(jnp.int32, (count, count), 0) == lax.broadcasted_iota(jnp.int32, (count, count), 1)
        lane = lax.broadcasted_iota(jnp.int32, (count, LANES), 1)
        table = jnp.zeros((count, LANES), F32)
        for e in range(n):
            line = first_w * (route_v[0:1, :] == e).astype(F32) + second_w * (route_v[1:2, :] == e).astype(F32)
            column = jnp.sum(jnp.where(eye, jnp.broadcast_to(line, (count, count)), 0.0), axis=1, keepdims=True)
            table = jnp.where(lane == e, jnp.broadcast_to(column, (count, LANES)), table)
        pack[:, depth:] = table.astype(BF16)
        token_own().start()
        for d in range(1, n):
            token_out(d).start()

    def share_tokens():
        for d in range(1, n):
            source = lax.rem(f + d, n)
            token_in(source).wait_recv()
            token_over(source).start()
            token_mate(source, 0).start()

    def pair_tokens():
        for d in range(1, n):
            source = lax.rem(f + d, n)
            token_from_over(source).wait_recv()
            token_mate(source, 1).start()

    def produce(i):
        for k in order:
            load(i, k, own_row).wait()
            fold(i % LOADS, k, own_row(i % CHUNKS), stage.at[k, i])
            if i + LOADS < items:
                load(i + LOADS, k, own_row).start()

            @pl.when(home)
            def _():
                if k == 0:
                    own_home(i).start()
                else:
                    first_home(k, i).start()

            if k >= 2:
                @pl.when(jnp.logical_not(home))
                def _():
                    first(k, i).start()

    def own(i, where):
        @pl.when(where)
        def _():
            direct(0, i).start()
            direct(1, i).start()

    def relay_home(i):
        for k in (2, 3):
            @pl.when(peers[k] == f)
            def _():
                first_home(k, i).wait_recv()
                across(f, i).start()

    def relay_near(i):
        for k in (2, 3):
            @pl.when(peers[k] == near)
            def _():
                first(k, i).wait_recv()
                layer(k, i).start()

    def relay_far(i, where):
        for k in (2, 3):
            @pl.when(where & (peers[k] != f) & (peers[k] != near))
            def _():
                first(k, i).wait_recv()
                layer(k, i).start()

    def turn(source, i):
        layer_in(source, i).wait_recv()
        across(source, i).start()

    def down_step(c):
        for k in order:
            load_d(k, c).wait()
            stage_d[k, c] = wide_d[c % DOWN_LOADS, k].astype(BF16)
            if c + DOWN_LOADS < DOWN_CHUNKS:
                load_d(k, c + DOWN_LOADS).start()
            down(k, c).start()

    def home_step(i):
        for k in (0, 1):
            load(i, k, other_row).wait()
            fold(i % LOADS, k, other_row(i % CHUNKS), extra.at[k, i])
            if i + LOADS < items:
                load(i + LOADS, k, other_row).start()
            (extra_home if k == 0 else extra_mate)(i).start()

    outer = (f == 0) | (f == n - 1)
    inner = jnp.logical_not(outer)
    own_far = (t != near) & jnp.logical_not(home)
    send_tokens()
    for i in range(items):
        produce(i)
        own(i, t == near)
        own(i, own_far & inner)
        if i < OUTER_LEAD:
            own(i, own_far & outer)
        if i == 1:
            for c in range(DOWN_LOADS):
                for k in order:
                    load_d(k, c).start()
    sent = {"own": OUTER_LEAD, "relay": 0, "near": 0, "in": 0, "out": 0}

    def up_to(name, limit, act):
        while sent[name] < min(limit, items):
            act(sent[name])
            sent[name] += 1

    for s in range(STEPS):
        if s < items:
            relay_home(s)
            relay_near(s)
            relay_far(s, inner)
        up_to("own", OUTER_LEAD + OUTER_OWN[min(s, len(OUTER_OWN) - 1)], lambda i: own(i, own_far & outer))
        up_to("relay", OUTER_RELAY[min(s, len(OUTER_RELAY) - 1)], lambda i: relay_far(i, outer))
        if s == 0:
            share_tokens()
        if 1 <= s <= DOWN_CHUNKS:
            down_step(s - 1)
        if s == items + 1:
            pair_tokens()
        up_to("near", s + 1 - NEAR_LAG, lambda i: turn(near, i))
        up_to("in", int((s + 1) * IN_RATE - IN_LAG), lambda i: turn(far[0], i))
        up_to("out", int((s + 1) * OUT_RATE - OUT_LAG), lambda i: turn(far[1], i))
        if s == items:
            @pl.when(home)
            def _():
                for j in range(LOADS):
                    for k in (0, 1):
                        load(j, k, other_row).start()
                for j in range(items):
                    home_step(j)
    assert min(sent.values()) == items

    def finish(i):
        @pl.when(home)
        def _():
            own_home(i).wait()
            extra_home(i).wait()
            extra_mate(i).wait_send()
            first_home(1, i).wait_send()

        @pl.when(jnp.logical_not(home))
        def _():
            direct(0, i).wait_send()
            direct(1, i).wait_send()

        @pl.when(f == mate)
        def _():
            first_home(1, i).wait_recv()
            extra_mate(i).wait_recv()

        for k in (2, 3):
            first(k, i).wait_send()

            @pl.when(peers[k] != f)
            def _():
                layer(k, i).wait_send()

            @pl.when(peers[k] == f)
            def _():
                across(f, i).wait()

        for source in (near, *far):
            across(source, i).wait()

    for i in range(items):
        finish(i)

    def finish_d(c, _):
        for k in range(n):
            down(k, c).wait()
        return 0

    lax.fori_loop(0, DOWN_CHUNKS, finish_d, 0)
    token_own().wait()
    for d in range(1, n):
        source = lax.rem(f + d, n)
        token_out(d).wait_send()
        token_over(source).wait_send()
        for j in range(2):
            token_mate(source, j).wait_send()
            token_from_mate(source, j).wait_recv()


def move(groups, n, tokens, routes, route_logits, gain, w_gate, w_up, w_down):
    experts, rows, cols = w_gate.shape
    hidden, width = w_down.shape[1:]
    count, depth = tokens.shape
    ch = rows // groups // CHUNKS
    dh = hidden // DOWN_CHUNKS
    items = 2 * CHUNKS
    dma = pltpu.SemaphoreType.DMA
    hbm = pl.BlockSpec(memory_space=pl.ANY)
    return pl.pallas_call(
        functools.partial(move_kernel, groups, n),
        out_shape=(
            pltpu.VMEM((count * n, depth + LANES), BF16),
            pltpu.VMEM((rows * n, cols), BF16),
            pltpu.VMEM((rows * n, cols), BF16),
            pltpu.VMEM((hidden, width * n), BF16),
        ),
        in_specs=[hbm] * 7,
        out_specs=(pl.BlockSpec(memory_space=pltpu.VMEM),) * 4,
        scratch_shapes=[
            pltpu.VMEM((LOADS, n, ch, cols), F32),
            pltpu.VMEM((DOWN_LOADS, n, dh, width), F32),
            pltpu.VMEM((n, items, ch, cols), BF16),
            pltpu.VMEM((2, items, ch, cols), BF16),
            pltpu.VMEM((2, items, ch, cols), BF16),
            pltpu.VMEM((n, DOWN_CHUNKS, dh, width), BF16),
            pltpu.VMEM((count, depth), BF16),
            pltpu.VMEM((count, depth + LANES), BF16),
            pltpu.VMEM((2, count), jnp.int32),
            pltpu.VMEM((2, count), F32),
            pltpu.VMEM((1, rows), F32),
            pltpu.VMEM((rows, LANES), F32),
            dma((LOADS, n)),
            dma((DOWN_LOADS, n)),
            dma((4,)),
            dma((n, items)),
            dma((n, items)),
            dma((2, items)),
            dma((items,)),
            dma((n, items)),
            dma((n, items)),
            dma((n, items)),
            dma((n, items)),
            dma((n, DOWN_CHUNKS)),
            dma((n, DOWN_CHUNKS)),
            dma((n,)),
            dma((n,)),
            dma((n,)),
            dma((n,)),
            dma((2, n)),
            dma((2, n)),
            dma((1,)),
        ],
        name="move_weights",
        compiler_params=pltpu.CompilerParams(
            collective_id=0, has_side_effects=True, vmem_limit_bytes=40 << 20
        ),
    )(tokens, routes.T, route_logits.T, gain.reshape(1, rows), w_gate, w_up, w_down)


def mix_kernel(tile, x_ref, gate_ref, up_ref, down_ref, gate_out, up_out, down_out, term_ref, total, out_sem):
    copies = [
        pltpu.make_async_copy(src, dst, out_sem.at[i])
        for i, (src, dst) in enumerate(((gate_ref, gate_out), (up_ref, up_out), (down_ref, down_out)))
    ]
    for copy in copies:
        copy.start()
    depth = gate_ref.shape[0]
    lane = lax.broadcasted_iota(jnp.int32, (x_ref.shape[0], LANES), 1)
    table = jnp.where(lane == lax.axis_index("tp"), x_ref[:, depth:].astype(F32), 0.0)
    scale = jnp.sum(table, axis=1, keepdims=True)
    total[...] = jnp.zeros_like(total)

    def trip(j, _):
        cols = pl.ds(pl.multiple_of(j * tile, tile), tile)
        x = x_ref[:, :depth]
        gate_act = jnp.dot(x, gate_ref[:, cols], preferred_element_type=F32)
        up_act = jnp.dot(x, up_ref[:, cols], preferred_element_type=F32)
        hidden = (gate_act / (1.0 + jnp.exp(-gate_act)) * up_act * scale).astype(BF16)
        total[...] += jnp.dot(hidden, down_ref[cols, :], preferred_element_type=F32)
        return 0

    lax.fori_loop(0, gate_ref.shape[1] // tile, trip, 0)
    term_ref[...] = total[...].astype(BF16)
    for copy in copies:
        copy.wait()


def mix(packed, gate, up, down):
    count = packed.shape[0]
    cols = gate.shape[1]
    wide = down.shape[1]
    tile = next(w for w in (256, 128) if cols % w == 0)
    vmem = pl.BlockSpec(memory_space=pltpu.VMEM)
    hbm = pl.BlockSpec(memory_space=pl.ANY)
    return pl.pallas_call(
        functools.partial(mix_kernel, tile),
        out_shape=(
            jax.ShapeDtypeStruct(gate.shape, BF16),
            jax.ShapeDtypeStruct(up.shape, BF16),
            jax.ShapeDtypeStruct(down.shape, BF16),
            pltpu.VMEM((count, wide), BF16),
        ),
        in_specs=[vmem] * 4,
        out_specs=(hbm, hbm, hbm, vmem),
        scratch_shapes=[pltpu.VMEM((count, wide), F32), pltpu.SemaphoreType.DMA((3,))],
        name="mix_tokens",
        compiler_params=pltpu.CompilerParams(vmem_limit_bytes=12 << 20),
    )(packed, gate, up, down)


def sum_kernel(n, term_ref, out_ref, near, near_in, far, far_in, last, last_in, s1, r1, s2, r2, s3, r3):
    g, f, t = lax.axis_index("grp"), lax.axis_index("fs"), lax.axis_index("tp")
    mesh_id = pl.DeviceIdType.MESH
    width = out_ref.shape[1]
    count = out_ref.shape[0]
    mate = t + 1 - 2 * lax.rem(t, 2)
    over = lax.rem(t + 2, n)
    mate_over = lax.rem(mate + 2, n)

    barrier = pltpu.get_barrier_semaphore()
    for e in (mate, over):
        pl.semaphore_signal(barrier, inc=1, device_id=(g, f, e), device_id_type=mesh_id)
    for d in range(1, n):
        pl.semaphore_signal(barrier, inc=1, device_id=(g, lax.rem(f + d, n), t), device_id_type=mesh_id)
    pl.semaphore_wait(barrier, n + 1)

    def block(layer, column):
        return term_ref.at[pl.ds(pl.multiple_of(layer * count, count), count), pl.ds(pl.multiple_of(column * width, width), width)]

    def remote(src, dst, ssem, rsem, where):
        return pltpu.make_async_remote_copy(
            src_ref=src, dst_ref=dst, send_sem=ssem, recv_sem=rsem, device_id=where, device_id_type=mesh_id
        )

    layers = [lax.rem(f + d, n) for d in (2, 1, 3, 0)]

    def to_mate(i, h):
        column = mate_over if h == 0 else mate
        return remote(block(layers[i], column), near_in.at[h, i], s1.at[h, i], r1.at[h, i], (g, f, mate))

    def to_over(i):
        return remote(far.at[i], far_in.at[i], s2.at[i], r2.at[i], (g, f, over))

    def to_layer(i):
        return remote(last.at[i], last_in.at[f], s3.at[i], r3.at[f], (g, layers[i], t))

    def from_layer(layer):
        return remote(last.at[0], last_in.at[layer], s3.at[0], r3.at[layer], (g, layer, t))

    for i in range(n):
        for h in range(2):
            to_mate(i, h).start()
    for i in range(n):
        to_mate(i, 0).wait_recv()
        far[i] = (block(layers[i], over)[...].astype(F32) + near_in[0, i].astype(F32)).astype(BF16)
        to_mate(i, 1).wait_recv()
        near[i] = block(layers[i], t)[...].astype(F32) + near_in[1, i].astype(F32)
        to_over(i).start()
    for i in range(n):
        to_over(i).wait_recv()
        near[i] = near[i] + far_in[i].astype(F32)
        if i < n - 1:
            last[i] = near[i].astype(BF16)
            to_layer(i).start()
    total = near[n - 1]
    for d in range(1, n):
        layer = lax.rem(f + d, n)
        from_layer(layer).wait_recv()
        total = total + last_in[layer].astype(F32)
    out_ref[...] = total.astype(BF16)
    for i in range(n):
        for h in range(2):
            to_mate(i, h).wait_send()
        to_over(i).wait_send()
        if i < n - 1:
            to_layer(i).wait_send()


def sum_terms(n, term):
    count, width = term.shape[0] // n, term.shape[1] // n
    dma = pltpu.SemaphoreType.DMA
    vmem = pl.BlockSpec(memory_space=pltpu.VMEM)
    piece = (count, width)
    return pl.pallas_call(
        functools.partial(sum_kernel, n),
        out_shape=jax.ShapeDtypeStruct(piece, BF16),
        in_specs=[vmem],
        out_specs=vmem,
        scratch_shapes=[
            pltpu.VMEM((n, *piece), F32),
            pltpu.VMEM((2, n, *piece), BF16),
            pltpu.VMEM((n, *piece), BF16),
            pltpu.VMEM((n, *piece), BF16),
            pltpu.VMEM((n, *piece), BF16),
            pltpu.VMEM((n, *piece), BF16),
            dma((2, n)), dma((2, n)), dma((n,)), dma((n,)), dma((n,)), dma((n,)),
        ],
        name="sum_terms",
        compiler_params=pltpu.CompilerParams(collective_id=1, has_side_effects=True, vmem_limit_bytes=8 << 20),
    )(term)


def fits(mesh, tokens, w_gate, w_down):
    groups, n, tp = mesh.shape["grp"], mesh.shape["fs"], mesh.shape["tp"]
    rows, cols = w_gate.shape[1:]
    hidden, width = w_down.shape[1:]
    return (
        groups == 2 and n == 4 and tp == 4 and w_gate.shape[0] == tp
        and cols == hidden and cols % 128 == 0 and width % 128 == 0 and tokens.shape[0] % (16 * n) == 0
        and rows % (groups * CHUNKS * 16) == 0 and hidden % (DOWN_CHUNKS * 16) == 0
        and tokens.shape[0] * n <= 512 and rows % LANES == 0 and rows * n == tokens.shape[1]
    )


def body(mesh, tokens, routes, route_logits, gain, w_gate, w_up, w_down):
    n, depth = mesh.shape["fs"], tokens.shape[1]
    if fits(mesh, tokens, w_gate, w_down):
        packed, gate, up, down = move(mesh.shape["grp"], n, tokens, routes, route_logits, gain, w_gate, w_up, w_down)
        gate, up, down, term = mix(packed, gate, up, down)
        return gate[None], up[None], down[None], sum_terms(n, term)
    values = tokens.astype(F32)
    mean_square = jnp.mean(values * values, axis=-1, keepdims=True)
    normed = (values * lax.rsqrt(mean_square + 1e-06)).astype(BF16)
    expert_id = lax.axis_index("tp")
    first = jax.nn.sigmoid(route_logits[:, 0] - route_logits[:, 1])
    second = jax.nn.sigmoid(route_logits[:, 1] - route_logits[:, 0])
    weight_col = first * (routes[:, 0] == expert_id).astype(F32)
    weight_col = (weight_col + second * (routes[:, 1] == expert_id).astype(F32)).astype(BF16)
    packed = jnp.concatenate([normed, jnp.broadcast_to(weight_col[:, None], (normed.shape[0], 128))], axis=1)
    packed = lax.all_gather(packed, "fs", axis=0, tiled=True)
    gate = (w_gate * gain[None, :, None]).astype(BF16)
    up = (w_up * gain[None, :, None]).astype(BF16)
    spread = functools.partial(lax.all_to_all, axis_name="tp", split_axis=0, concat_axis=2, tiled=True)
    gate, up, down = spread(gate), spread(up), spread(w_down.astype(BF16))
    stack = functools.partial(lax.all_to_all, axis_name="fs", split_axis=2, concat_axis=1, tiled=True)
    gate, up = stack(gate), stack(up)
    rows, weight = packed[:, :depth], packed[:, depth : depth + 1]
    gate_act = jnp.dot(rows, gate[0], preferred_element_type=F32)
    up_act = jnp.dot(rows, up[0], preferred_element_type=F32)
    hidden = (jax.nn.silu(gate_act) * up_act * weight.astype(F32)).astype(BF16)
    term = jnp.dot(hidden, down[0], preferred_element_type=F32)
    by_feature = lax.psum_scatter(term, "tp", scatter_dimension=1, tiled=True)
    mixed = lax.psum_scatter(by_feature, "fs", scatter_dimension=0, tiled=True)
    return gate, up, down, mixed.astype(BF16)


def solution(mesh):
    return jax.shard_map(
        functools.partial(body, mesh),
        mesh=mesh,
        in_specs=(
            P(("grp", "fs"), None),
            P(("grp", "fs"), None),
            P(("grp", "fs"), None),
            P("fs"),
            P(None, "fs", "tp"),
            P(None, "fs", "tp"),
            P(None, "fs", "tp"),
        ),
        out_specs=(
            P(("grp", "tp"), None, "fs"),
            P(("grp", "tp"), None, "fs"),
            P(("grp", "tp"), "fs", None),
            P(("grp", "fs"), "tp"),
        ),
        check_vma=False,
    )
```

```python
import functools

import jax
import jax.numpy as jnp
from jax import lax
from jax.experimental import pallas as pl
from jax.experimental.pallas import tpu as pltpu
from jax.sharding import PartitionSpec as P

BF16 = jnp.bfloat16
F32 = jnp.float32
CHUNKS = 8
DOWN_CHUNKS = 4
LOADS = 4
DOWN_LOADS = 2
AHEAD = 6
DOWN_STEPS = (-3, 0, 4, 8)
INNER_LEAD = 1
OUTER_LEAD = 1
FAR_RATE = 0.5
SEND_RATE = 0.55
NEAR_LAG = 2
IN_LAG = 2
OUT_LAG = 2.5
LANES = 128


def move_kernel(
    groups, n, tokens_ref, routes_ref, logits_ref, gain_ref, wg_ref, wu_ref, wd_ref, x_ref, og_ref, ou_ref, od_ref,
    wide, wide_d, stage, extra, relay, stage_d, tok, pack, route_v, logit_v, gain_v, gain_col,
    load_sem, load_d_sem, small_sem, s1s, s1r, xs, xr, zs, zr, ys, yr, ds, dr, ts, tr, os, ov, ms, mr, own_sem,
):
    g, f, t = lax.axis_index("grp"), lax.axis_index("fs"), lax.axis_index("tp")
    rows = wg_ref.shape[1]
    half = rows // groups
    ch = half // CHUNKS
    hidden, width = wd_ref.shape[1:]
    dh = hidden // DOWN_CHUNKS
    items = 2 * CHUNKS
    count, depth = tokens_ref.shape
    part = count // n
    weights = (wg_ref, wu_ref)

    core = lax.rem(t, 2)
    mate = t + 1 - 2 * core
    peers = (t, mate, lax.rem(t + 2, n), lax.rem(mate + 2, n))
    home = f == t
    order = (2, 3, 0, 1)
    near = f + 1 - 2 * lax.rem(f, 2)
    low = f < n // 2
    far = (jnp.where(low, 2, 1), jnp.where(low, 3, 0))

    def remote(src, dst, ssem, rsem, where):
        return pltpu.make_async_remote_copy(
            src_ref=src, dst_ref=dst, send_sem=ssem, recv_sem=rsem,
            device_id=where, device_id_type=pl.DeviceIdType.MESH,
        )

    def own_row(c):
        return pl.multiple_of(g * half + c * ch, ch)

    def other_row(c):
        return pl.multiple_of((1 - g) * half + c * ch, ch)

    def load(i, k, row):
        slot = i % LOADS
        src = weights[i // CHUNKS].at[peers[k], pl.ds(row(i % CHUNKS), ch), :]
        return pltpu.make_async_copy(src, wide.at[slot, k], load_sem.at[slot, k])

    for i in range(LOADS):
        for k in order:
            load(i, k, own_row).start()
    small = (
        pltpu.make_async_copy(gain_ref, gain_v, small_sem.at[0]),
        pltpu.make_async_copy(tokens_ref, tok, small_sem.at[1]),
        pltpu.make_async_copy(routes_ref, route_v, small_sem.at[2]),
        pltpu.make_async_copy(logits_ref, logit_v, small_sem.at[3]),
    )
    for copy in small:
        copy.start()

    barrier = pltpu.get_barrier_semaphore()

    def greet(where):
        pl.semaphore_signal(barrier, inc=1, device_id=where, device_id_type=pl.DeviceIdType.MESH)

    for k in (1, 2, 3):
        greet((g, f, peers[k]))
    for d in range(1, n):
        for k in (0, 1):
            greet((g, lax.rem(f + d, n), peers[k]))
    greet((1 - g, f, t))

    small[0].wait()
    for b in range(rows // LANES):
        line = gain_v[0:1, b * LANES : (b + 1) * LANES]
        eye = lax.broadcasted_iota(jnp.int32, (LANES, LANES), 0) == lax.broadcasted_iota(jnp.int32, (LANES, LANES), 1)
        column = jnp.sum(jnp.where(eye, jnp.broadcast_to(line, (LANES, LANES)), 0.0), axis=1, keepdims=True)
        gain_col[b * LANES : (b + 1) * LANES, :] = jnp.broadcast_to(column, (LANES, LANES))
    pl.semaphore_wait(barrier, 2 * n + 2)

    def at_rows(i, source, row):
        return (og_ref, ou_ref)[i // CHUNKS].at[pl.ds(pl.multiple_of(source * rows + row, ch), ch), :]

    def own_piece(i, source):
        return at_rows(i, source, own_row(i % CHUNKS))

    def other_piece(i, source):
        return at_rows(i, source, other_row(i % CHUNKS))

    def first(k, i):
        return remote(stage.at[k, i], relay.at[k - 2, i], s1s.at[k, i], s1r.at[k, i], (g, f, peers[k]))

    def first_home(k, i):
        return remote(stage.at[k, i], own_piece(i, f), s1s.at[k, i], s1r.at[k, i], (g, f, peers[k]))

    def own_home(i):
        return pltpu.make_async_copy(stage.at[0, i], own_piece(i, f), s1s.at[0, i])

    def direct(k, i):
        return remote(stage.at[k, i], own_piece(i, f), zs.at[k, i], zr.at[f, i], (g, t, peers[k]))

    def layer(k, i):
        return remote(relay.at[k - 2, i], own_piece(i, f), zs.at[k, i], zr.at[f, i], (g, peers[k], t))

    def layer_in(source, i):
        piece = own_piece(i, source)
        return remote(piece, piece, zs.at[0, i], zr.at[source, i], (1 - g, f, t))

    def across(source, i):
        piece = own_piece(i, source)
        return remote(piece, piece, ys.at[source, i], yr.at[source, i], (1 - g, f, t))

    def extra_home(i):
        return pltpu.make_async_copy(extra.at[0, i], other_piece(i, f), xs.at[0, i])

    def extra_mate(i):
        return remote(extra.at[1, i], other_piece(i, f), xs.at[1, i], xr.at[i], (g, f, mate))

    def down(k, c):
        src = stage_d.at[k, c]
        dst = od_ref.at[pl.ds(c * dh, dh), pl.ds(pl.multiple_of(t * width, LANES), width)]
        if k == 0:
            return pltpu.make_async_copy(src, dst, ds.at[0, c])
        return remote(src, dst, ds.at[k, c], dr.at[k, c], (g, f, peers[k]))

    def load_d(k, c):
        slot = c % DOWN_LOADS
        return pltpu.make_async_copy(wd_ref.at[peers[k], pl.ds(c * dh, dh), :], wide_d.at[slot, k], load_d_sem.at[slot, k])

    def fold(slot, k, row, dst):
        scale = gain_col[pl.ds(row, ch), 0:1]
        dst[...] = (wide[slot, k] * scale).astype(BF16)

    def piece(source, q):
        return x_ref.at[pl.ds(pl.multiple_of(source * count + q * part, part), part), :]

    def token_out(d):
        src = pack.at[pl.ds(pl.multiple_of(t * part, part), part), :]
        return remote(src, piece(f, t), ts.at[d], tr.at[f], (g, lax.rem(f + d, n), t))

    def token_in(source):
        return remote(piece(source, t), piece(source, t), ts.at[0], tr.at[source], (g, f, t))

    def token_over(source):
        here = piece(source, t)
        return remote(here, here, os.at[source], ov.at[source], (g, f, peers[2]))

    def token_from_over(source):
        here = piece(source, peers[2])
        return remote(here, here, os.at[source], ov.at[source], (g, f, peers[2]))

    def token_mate(source, j):
        here = piece(source, (t, peers[2])[j])
        return remote(here, here, ms.at[j, source], mr.at[j, source], (g, f, mate))

    def token_from_mate(source, j):
        here = piece(source, (mate, peers[3])[j])
        return remote(here, here, ms.at[j, source], mr.at[j, source], (g, f, mate))

    def token_own():
        return pltpu.make_async_copy(pack, x_ref.at[pl.ds(pl.multiple_of(f * count, count), count), :], own_sem.at[0])

    def send_tokens():
        for copy in small[1:]:
            copy.wait()
        values = tok[...].astype(F32)
        mean_square = jnp.mean(values * values, axis=-1, keepdims=True)
        pack[:, :depth] = (values * lax.rsqrt(mean_square + 1e-06)).astype(BF16)
        diff = logit_v[0:1, :] - logit_v[1:2, :]
        first_w = 1.0 / (1.0 + jnp.exp(-diff))
        second_w = 1.0 / (1.0 + jnp.exp(diff))
        eye = lax.broadcasted_iota(jnp.int32, (count, count), 0) == lax.broadcasted_iota(jnp.int32, (count, count), 1)
        lane = lax.broadcasted_iota(jnp.int32, (count, LANES), 1)
        table = jnp.zeros((count, LANES), F32)
        for e in range(n):
            line = first_w * (route_v[0:1, :] == e).astype(F32) + second_w * (route_v[1:2, :] == e).astype(F32)
            column = jnp.sum(jnp.where(eye, jnp.broadcast_to(line, (count, count)), 0.0), axis=1, keepdims=True)
            table = jnp.where(lane == e, jnp.broadcast_to(column, (count, LANES)), table)
        pack[:, depth:] = table.astype(BF16)
        token_own().start()
        for d in range(1, n):
            token_out(d).start()

    def share_tokens():
        for d in range(1, n):
            source = lax.rem(f + d, n)
            token_in(source).wait_recv()
            token_over(source).start()
            token_mate(source, 0).start()

    def pair_tokens():
        for d in range(1, n):
            source = lax.rem(f + d, n)
            token_from_over(source).wait_recv()
            token_mate(source, 1).start()

    def produce(i):
        for k in order:
            load(i, k, own_row).wait()
            fold(i % LOADS, k, own_row(i % CHUNKS), stage.at[k, i])
            if i + LOADS < items:
                load(i + LOADS, k, own_row).start()

            @pl.when(home)
            def _():
                if k == 0:
                    own_home(i).start()
                else:
                    first_home(k, i).start()

            if k >= 2:
                @pl.when(jnp.logical_not(home))
                def _():
                    first(k, i).start()

    def own(i, where):
        @pl.when(where)
        def _():
            direct(0, i).start()
            direct(1, i).start()

    def relay_home(i):
        for k in (2, 3):
            @pl.when(peers[k] == f)
            def _():
                first_home(k, i).wait_recv()
                across(f, i).start()

    def relay_near(i):
        for k in (2, 3):
            @pl.when(peers[k] == near)
            def _():
                first(k, i).wait_recv()
                layer(k, i).start()

    def relay_far(i, where):
        for k in (2, 3):
            @pl.when(where & (peers[k] != f) & (peers[k] != near))
            def _():
                first(k, i).wait_recv()
                layer(k, i).start()

    def turn(source, i):
        layer_in(source, i).wait_recv()
        across(source, i).start()

    def down_step(c):
        for k in order:
            load_d(k, c).wait()
            stage_d[k, c] = wide_d[c % DOWN_LOADS, k].astype(BF16)
            if c + DOWN_LOADS < DOWN_CHUNKS:
                load_d(k, c + DOWN_LOADS).start()
            down(k, c).start()

    def home_step(i):
        for k in (0, 1):
            load(i, k, other_row).wait()
            fold(i % LOADS, k, other_row(i % CHUNKS), extra.at[k, i])
            if i + LOADS < items:
                load(i + LOADS, k, other_row).start()
            (extra_home if k == 0 else extra_mate)(i).start()

    outer = (f == 0) | (f == n - 1)
    inner = jnp.logical_not(outer)
    own_far = (t != near) & jnp.logical_not(home)
    send_tokens()
    for c in range(DOWN_LOADS):
        for k in order:
            load_d(k, c).start()
    sent = dict.fromkeys(("item", "inner own", "inner relay", "outer own", "outer relay", "near", "in", "out", "down"), 0)

    def start_item(i):
        produce(i)
        own(i, t == near)

    def up_to(name, limit, act):
        while sent[name] < min(limit, items):
            act(sent[name])
            sent[name] += 1

    sent["down"] = items - DOWN_CHUNKS
    s = 0
    while min(sent.values()) < items:
        paced = int(s * SEND_RATE)
        up_to("item", s + AHEAD, start_item)
        made = sent["item"]
        up_to("inner own", min(made, INNER_LEAD + paced), lambda i: own(i, own_far & inner))
        up_to("outer own", min(made, OUTER_LEAD + paced), lambda i: own(i, own_far & outer))
        if s < items:
            relay_home(s)
            relay_near(s)
        up_to("inner relay", min(s + 1, INNER_LEAD + paced), lambda i: relay_far(i, inner))
        up_to("outer relay", min(s + 1, OUTER_LEAD + paced), lambda i: relay_far(i, outer))
        if s == 0:
            share_tokens()
        if s == items + 1:
            pair_tokens()
        if s - items in DOWN_STEPS:
            down_step(DOWN_STEPS.index(s - items))
            sent["down"] += 1
        up_to("near", s + 1 - NEAR_LAG, lambda i: turn(near, i))
        up_to("in", int((s + 1 - IN_LAG) * FAR_RATE), lambda i: turn(far[0], i))
        up_to("out", int((s + 1 - OUT_LAG) * FAR_RATE), lambda i: turn(far[1], i))
        if s == items + 2:
            @pl.when(home)
            def _():
                for j in range(LOADS):
                    for k in (0, 1):
                        load(j, k, other_row).start()
                for j in range(items):
                    home_step(j)
        s += 1

    def finish(i):
        @pl.when(home)
        def _():
            own_home(i).wait()
            extra_home(i).wait()
            extra_mate(i).wait_send()
            first_home(1, i).wait_send()

        @pl.when(jnp.logical_not(home))
        def _():
            direct(0, i).wait_send()
            direct(1, i).wait_send()

        @pl.when(f == mate)
        def _():
            first_home(1, i).wait_recv()
            extra_mate(i).wait_recv()

        for k in (2, 3):
            first(k, i).wait_send()

            @pl.when(peers[k] != f)
            def _():
                layer(k, i).wait_send()

            @pl.when(peers[k] == f)
            def _():
                across(f, i).wait()

        for source in (near, *far):
            across(source, i).wait()

    for i in range(items):
        finish(i)

    def finish_d(c, _):
        for k in range(n):
            down(k, c).wait()
        return 0

    lax.fori_loop(0, DOWN_CHUNKS, finish_d, 0)
    token_own().wait()
    for d in range(1, n):
        source = lax.rem(f + d, n)
        token_out(d).wait_send()
        token_over(source).wait_send()
        for j in range(2):
            token_mate(source, j).wait_send()
            token_from_mate(source, j).wait_recv()


def move(groups, n, tokens, routes, route_logits, gain, w_gate, w_up, w_down):
    experts, rows, cols = w_gate.shape
    hidden, width = w_down.shape[1:]
    count, depth = tokens.shape
    ch = rows // groups // CHUNKS
    dh = hidden // DOWN_CHUNKS
    items = 2 * CHUNKS
    dma = pltpu.SemaphoreType.DMA
    hbm = pl.BlockSpec(memory_space=pl.ANY)
    return pl.pallas_call(
        functools.partial(move_kernel, groups, n),
        out_shape=(
            pltpu.VMEM((count * n, depth + LANES), BF16),
            pltpu.VMEM((rows * n, cols), BF16),
            pltpu.VMEM((rows * n, cols), BF16),
            pltpu.VMEM((hidden, width * n), BF16),
        ),
        in_specs=[hbm] * 7,
        out_specs=(pl.BlockSpec(memory_space=pltpu.VMEM),) * 4,
        scratch_shapes=[
            pltpu.VMEM((LOADS, n, ch, cols), F32),
            pltpu.VMEM((DOWN_LOADS, n, dh, width), F32),
            pltpu.VMEM((n, items, ch, cols), BF16),
            pltpu.VMEM((2, items, ch, cols), BF16),
            pltpu.VMEM((2, items, ch, cols), BF16),
            pltpu.VMEM((n, DOWN_CHUNKS, dh, width), BF16),
            pltpu.VMEM((count, depth), BF16),
            pltpu.VMEM((count, depth + LANES), BF16),
            pltpu.VMEM((2, count), jnp.int32),
            pltpu.VMEM((2, count), F32),
            pltpu.VMEM((1, rows), F32),
            pltpu.VMEM((rows, LANES), F32),
            dma((LOADS, n)),
            dma((DOWN_LOADS, n)),
            dma((4,)),
            dma((n, items)),
            dma((n, items)),
            dma((2, items)),
            dma((items,)),
            dma((n, items)),
            dma((n, items)),
            dma((n, items)),
            dma((n, items)),
            dma((n, DOWN_CHUNKS)),
            dma((n, DOWN_CHUNKS)),
            dma((n,)),
            dma((n,)),
            dma((n,)),
            dma((n,)),
            dma((2, n)),
            dma((2, n)),
            dma((1,)),
        ],
        name="move_weights",
        compiler_params=pltpu.CompilerParams(
            collective_id=0, has_side_effects=True, vmem_limit_bytes=40 << 20
        ),
    )(tokens, routes.T, route_logits.T, gain.reshape(1, rows), w_gate, w_up, w_down)


def mix_kernel(tile, x_ref, gate_ref, up_ref, down_ref, gate_out, up_out, down_out, term_ref, total, out_sem):
    copies = [
        pltpu.make_async_copy(src, dst, out_sem.at[i])
        for i, (src, dst) in enumerate(((gate_ref, gate_out), (up_ref, up_out), (down_ref, down_out)))
    ]
    for copy in copies:
        copy.start()
    depth = gate_ref.shape[0]
    lane = lax.broadcasted_iota(jnp.int32, (x_ref.shape[0], LANES), 1)
    table = jnp.where(lane == lax.axis_index("tp"), x_ref[:, depth:].astype(F32), 0.0)
    scale = jnp.sum(table, axis=1, keepdims=True)
    total[...] = jnp.zeros_like(total)

    def trip(j, _):
        cols = pl.ds(pl.multiple_of(j * tile, tile), tile)
        x = x_ref[:, :depth]
        gate_act = jnp.dot(x, gate_ref[:, cols], preferred_element_type=F32)
        up_act = jnp.dot(x, up_ref[:, cols], preferred_element_type=F32)
        hidden = (gate_act / (1.0 + jnp.exp(-gate_act)) * up_act * scale).astype(BF16)
        total[...] += jnp.dot(hidden, down_ref[cols, :], preferred_element_type=F32)
        return 0

    lax.fori_loop(0, gate_ref.shape[1] // tile, trip, 0)
    term_ref[...] = total[...].astype(BF16)
    for copy in copies:
        copy.wait()


def mix(packed, gate, up, down):
    count = packed.shape[0]
    cols = gate.shape[1]
    wide = down.shape[1]
    tile = next(w for w in (256, 128) if cols % w == 0)
    vmem = pl.BlockSpec(memory_space=pltpu.VMEM)
    hbm = pl.BlockSpec(memory_space=pl.ANY)
    return pl.pallas_call(
        functools.partial(mix_kernel, tile),
        out_shape=(
            jax.ShapeDtypeStruct(gate.shape, BF16),
            jax.ShapeDtypeStruct(up.shape, BF16),
            jax.ShapeDtypeStruct(down.shape, BF16),
            pltpu.VMEM((count, wide), BF16),
        ),
        in_specs=[vmem] * 4,
        out_specs=(hbm, hbm, hbm, vmem),
        scratch_shapes=[pltpu.VMEM((count, wide), F32), pltpu.SemaphoreType.DMA((3,))],
        name="mix_tokens",
        compiler_params=pltpu.CompilerParams(vmem_limit_bytes=12 << 20),
    )(packed, gate, up, down)


def sum_kernel(n, term_ref, out_ref, near, near_in, far, far_in, last, last_in, s1, r1, s2, r2, s3, r3):
    g, f, t = lax.axis_index("grp"), lax.axis_index("fs"), lax.axis_index("tp")
    mesh_id = pl.DeviceIdType.MESH
    width = out_ref.shape[1]
    count = out_ref.shape[0]
    mate = t + 1 - 2 * lax.rem(t, 2)
    over = lax.rem(t + 2, n)
    mate_over = lax.rem(mate + 2, n)

    barrier = pltpu.get_barrier_semaphore()
    for e in (mate, over):
        pl.semaphore_signal(barrier, inc=1, device_id=(g, f, e), device_id_type=mesh_id)
    for d in range(1, n):
        pl.semaphore_signal(barrier, inc=1, device_id=(g, lax.rem(f + d, n), t), device_id_type=mesh_id)
    pl.semaphore_wait(barrier, n + 1)

    def block(layer, column):
        return term_ref.at[pl.ds(pl.multiple_of(layer * count, count), count), pl.ds(pl.multiple_of(column * width, width), width)]

    def remote(src, dst, ssem, rsem, where):
        return pltpu.make_async_remote_copy(
            src_ref=src, dst_ref=dst, send_sem=ssem, recv_sem=rsem, device_id=where, device_id_type=mesh_id
        )

    layers = [lax.rem(f + d, n) for d in (2, 1, 3, 0)]

    def to_mate(i, h):
        column = mate_over if h == 0 else mate
        return remote(block(layers[i], column), near_in.at[h, i], s1.at[h, i], r1.at[h, i], (g, f, mate))

    def to_over(i):
        return remote(far.at[i], far_in.at[i], s2.at[i], r2.at[i], (g, f, over))

    def to_layer(i):
        return remote(last.at[i], last_in.at[f], s3.at[i], r3.at[f], (g, layers[i], t))

    def from_layer(layer):
        return remote(last.at[0], last_in.at[layer], s3.at[0], r3.at[layer], (g, layer, t))

    for i in range(n):
        for h in range(2):
            to_mate(i, h).start()
    for i in range(n):
        to_mate(i, 0).wait_recv()
        far[i] = (block(layers[i], over)[...].astype(F32) + near_in[0, i].astype(F32)).astype(BF16)
        to_mate(i, 1).wait_recv()
        near[i] = block(layers[i], t)[...].astype(F32) + near_in[1, i].astype(F32)
        to_over(i).start()
    for i in range(n):
        to_over(i).wait_recv()
        near[i] = near[i] + far_in[i].astype(F32)
        if i < n - 1:
            last[i] = near[i].astype(BF16)
            to_layer(i).start()
    total = near[n - 1]
    for d in range(1, n):
        layer = lax.rem(f + d, n)
        from_layer(layer).wait_recv()
        total = total + last_in[layer].astype(F32)
    out_ref[...] = total.astype(BF16)
    for i in range(n):
        for h in range(2):
            to_mate(i, h).wait_send()
        to_over(i).wait_send()
        if i < n - 1:
            to_layer(i).wait_send()


def sum_terms(n, term):
    count, width = term.shape[0] // n, term.shape[1] // n
    dma = pltpu.SemaphoreType.DMA
    vmem = pl.BlockSpec(memory_space=pltpu.VMEM)
    piece = (count, width)
    return pl.pallas_call(
        functools.partial(sum_kernel, n),
        out_shape=jax.ShapeDtypeStruct(piece, BF16),
        in_specs=[vmem],
        out_specs=vmem,
        scratch_shapes=[
            pltpu.VMEM((n, *piece), F32),
            pltpu.VMEM((2, n, *piece), BF16),
            pltpu.VMEM((n, *piece), BF16),
            pltpu.VMEM((n, *piece), BF16),
            pltpu.VMEM((n, *piece), BF16),
            pltpu.VMEM((n, *piece), BF16),
            dma((2, n)), dma((2, n)), dma((n,)), dma((n,)), dma((n,)), dma((n,)),
        ],
        name="sum_terms",
        compiler_params=pltpu.CompilerParams(collective_id=1, has_side_effects=True, vmem_limit_bytes=8 << 20),
    )(term)


def fits(mesh, tokens, w_gate, w_down):
    groups, n, tp = mesh.shape["grp"], mesh.shape["fs"], mesh.shape["tp"]
    rows, cols = w_gate.shape[1:]
    hidden, width = w_down.shape[1:]
    return (
        groups == 2 and n == 4 and tp == 4 and w_gate.shape[0] == tp
        and cols == hidden and cols % 128 == 0 and width % 128 == 0 and tokens.shape[0] % (16 * n) == 0
        and rows % (groups * CHUNKS * 16) == 0 and hidden % (DOWN_CHUNKS * 16) == 0
        and tokens.shape[0] * n <= 512 and rows % LANES == 0 and rows * n == tokens.shape[1]
    )


def body(mesh, tokens, routes, route_logits, gain, w_gate, w_up, w_down):
    n, depth = mesh.shape["fs"], tokens.shape[1]
    if fits(mesh, tokens, w_gate, w_down):
        packed, gate, up, down = move(mesh.shape["grp"], n, tokens, routes, route_logits, gain, w_gate, w_up, w_down)
        gate, up, down, term = mix(packed, gate, up, down)
        return gate[None], up[None], down[None], sum_terms(n, term)
    values = tokens.astype(F32)
    mean_square = jnp.mean(values * values, axis=-1, keepdims=True)
    normed = (values * lax.rsqrt(mean_square + 1e-06)).astype(BF16)
    expert_id = lax.axis_index("tp")
    first = jax.nn.sigmoid(route_logits[:, 0] - route_logits[:, 1])
    second = jax.nn.sigmoid(route_logits[:, 1] - route_logits[:, 0])
    weight_col = first * (routes[:, 0] == expert_id).astype(F32)
    weight_col = (weight_col + second * (routes[:, 1] == expert_id).astype(F32)).astype(BF16)
    packed = jnp.concatenate([normed, jnp.broadcast_to(weight_col[:, None], (normed.shape[0], 128))], axis=1)
    packed = lax.all_gather(packed, "fs", axis=0, tiled=True)
    gate = (w_gate * gain[None, :, None]).astype(BF16)
    up = (w_up * gain[None, :, None]).astype(BF16)
    spread = functools.partial(lax.all_to_all, axis_name="tp", split_axis=0, concat_axis=2, tiled=True)
    gate, up, down = spread(gate), spread(up), spread(w_down.astype(BF16))
    stack = functools.partial(lax.all_to_all, axis_name="fs", split_axis=2, concat_axis=1, tiled=True)
    gate, up = stack(gate), stack(up)
    rows, weight = packed[:, :depth], packed[:, depth : depth + 1]
    gate_act = jnp.dot(rows, gate[0], preferred_element_type=F32)
    up_act = jnp.dot(rows, up[0], preferred_element_type=F32)
    hidden = (jax.nn.silu(gate_act) * up_act * weight.astype(F32)).astype(BF16)
    term = jnp.dot(hidden, down[0], preferred_element_type=F32)
    by_feature = lax.psum_scatter(term, "tp", scatter_dimension=1, tiled=True)
    mixed = lax.psum_scatter(by_feature, "fs", scatter_dimension=0, tiled=True)
    return gate, up, down, mixed.astype(BF16)


def solution(mesh):
    return jax.shard_map(
        functools.partial(body, mesh),
        mesh=mesh,
        in_specs=(
            P(("grp", "fs"), None),
            P(("grp", "fs"), None),
            P(("grp", "fs"), None),
            P("fs"),
            P(None, "fs", "tp"),
            P(None, "fs", "tp"),
            P(None, "fs", "tp"),
        ),
        out_specs=(
            P(("grp", "tp"), None, "fs"),
            P(("grp", "tp"), None, "fs"),
            P(("grp", "tp"), "fs", None),
            P(("grp", "fs"), "tp"),
        ),
        check_vma=False,
    )
```

```python
import functools

import jax
import jax.numpy as jnp
from jax import lax
from jax.experimental import pallas as pl
from jax.experimental.pallas import tpu as pltpu
from jax.sharding import PartitionSpec as P

BF16 = jnp.bfloat16
F32 = jnp.float32
CHUNKS = 8
DOWN_CHUNKS = 4
LOADS = 4
DOWN_LOADS = 2
AHEAD = 6
DOWN_STEPS = (-5, -2, 1, 4)
INNER_LEAD = 2
OUTER_LEAD = 1
FAR_RATE = 0.5
SEND_RATE = 0.5
NEAR_LAG = 2
IN_LAG = 3
OUT_LAG = 2
LANES = 128


def move_kernel(
    groups, n, tokens_ref, routes_ref, logits_ref, gain_ref, wg_ref, wu_ref, wd_ref, x_ref, og_ref, ou_ref, od_ref,
    wide, wide_d, stage, extra, relay, stage_d, tok, pack, route_v, logit_v, gain_v, gain_col,
    load_sem, load_d_sem, small_sem, s1s, s1r, xs, xr, zs, zr, ys, yr, ds, dr, ts, tr, os, ov, ms, mr, own_sem,
):
    g, f, t = lax.axis_index("grp"), lax.axis_index("fs"), lax.axis_index("tp")
    rows = wg_ref.shape[1]
    half = rows // groups
    ch = half // CHUNKS
    hidden, width = wd_ref.shape[1:]
    dh = hidden // DOWN_CHUNKS
    items = 2 * CHUNKS
    count, depth = tokens_ref.shape
    part = count // n
    weights = (wg_ref, wu_ref)

    core = lax.rem(t, 2)
    mate = t + 1 - 2 * core
    peers = (t, mate, lax.rem(t + 2, n), lax.rem(mate + 2, n))
    home = f == t
    order = (2, 3, 0, 1)
    near = f + 1 - 2 * lax.rem(f, 2)
    low = f < n // 2
    far = (jnp.where(low, 2, 1), jnp.where(low, 3, 0))

    def remote(src, dst, ssem, rsem, where):
        return pltpu.make_async_remote_copy(
            src_ref=src, dst_ref=dst, send_sem=ssem, recv_sem=rsem,
            device_id=where, device_id_type=pl.DeviceIdType.MESH,
        )

    def own_row(c):
        return pl.multiple_of(g * half + c * ch, ch)

    def other_row(c):
        return pl.multiple_of((1 - g) * half + c * ch, ch)

    def load(i, k, row):
        slot = i % LOADS
        src = weights[i // CHUNKS].at[peers[k], pl.ds(row(i % CHUNKS), ch), :]
        return pltpu.make_async_copy(src, wide.at[slot, k], load_sem.at[slot, k])

    for i in range(LOADS):
        for k in order:
            load(i, k, own_row).start()
    small = (
        pltpu.make_async_copy(gain_ref, gain_v, small_sem.at[0]),
        pltpu.make_async_copy(tokens_ref, tok, small_sem.at[1]),
        pltpu.make_async_copy(routes_ref, route_v, small_sem.at[2]),
        pltpu.make_async_copy(logits_ref, logit_v, small_sem.at[3]),
    )
    for copy in small:
        copy.start()

    barrier = pltpu.get_barrier_semaphore()

    def greet(where):
        pl.semaphore_signal(barrier, inc=1, device_id=where, device_id_type=pl.DeviceIdType.MESH)

    for k in (1, 2, 3):
        greet((g, f, peers[k]))
    for d in range(1, n):
        for k in (0, 1):
            greet((g, lax.rem(f + d, n), peers[k]))
    greet((1 - g, f, t))

    small[0].wait()
    for b in range(rows // LANES):
        line = gain_v[0:1, b * LANES : (b + 1) * LANES]
        eye = lax.broadcasted_iota(jnp.int32, (LANES, LANES), 0) == lax.broadcasted_iota(jnp.int32, (LANES, LANES), 1)
        column = jnp.sum(jnp.where(eye, jnp.broadcast_to(line, (LANES, LANES)), 0.0), axis=1, keepdims=True)
        gain_col[b * LANES : (b + 1) * LANES, :] = jnp.broadcast_to(column, (LANES, LANES))
    pl.semaphore_wait(barrier, 2 * n + 2)

    def at_rows(i, source, row):
        return (og_ref, ou_ref)[i // CHUNKS].at[pl.ds(pl.multiple_of(source * rows + row, ch), ch), :]

    def own_piece(i, source):
        return at_rows(i, source, own_row(i % CHUNKS))

    def other_piece(i, source):
        return at_rows(i, source, other_row(i % CHUNKS))

    def first(k, i):
        return remote(stage.at[k, i], relay.at[k - 2, i], s1s.at[k, i], s1r.at[k, i], (g, f, peers[k]))

    def first_home(k, i):
        return remote(stage.at[k, i], own_piece(i, f), s1s.at[k, i], s1r.at[k, i], (g, f, peers[k]))

    def own_home(i):
        return pltpu.make_async_copy(stage.at[0, i], own_piece(i, f), s1s.at[0, i])

    def direct(k, i):
        return remote(stage.at[k, i], own_piece(i, f), zs.at[k, i], zr.at[f, i], (g, t, peers[k]))

    def layer(k, i):
        return remote(relay.at[k - 2, i], own_piece(i, f), zs.at[k, i], zr.at[f, i], (g, peers[k], t))

    def layer_in(source, i):
        piece = own_piece(i, source)
        return remote(piece, piece, zs.at[0, i], zr.at[source, i], (1 - g, f, t))

    def across(source, i):
        piece = own_piece(i, source)
        return remote(piece, piece, ys.at[source, i], yr.at[source, i], (1 - g, f, t))

    def extra_home(i):
        return pltpu.make_async_copy(extra.at[0, i], other_piece(i, f), xs.at[0, i])

    def extra_mate(i):
        return remote(extra.at[1, i], other_piece(i, f), xs.at[1, i], xr.at[i], (g, f, mate))

    def down(k, c):
        src = stage_d.at[k, c]
        dst = od_ref.at[pl.ds(c * dh, dh), pl.ds(pl.multiple_of(t * width, LANES), width)]
        if k == 0:
            return pltpu.make_async_copy(src, dst, ds.at[0, c])
        return remote(src, dst, ds.at[k, c], dr.at[k, c], (g, f, peers[k]))

    def load_d(k, c):
        slot = c % DOWN_LOADS
        return pltpu.make_async_copy(wd_ref.at[peers[k], pl.ds(c * dh, dh), :], wide_d.at[slot, k], load_d_sem.at[slot, k])

    def fold(slot, k, row, dst):
        scale = gain_col[pl.ds(row, ch), 0:1]
        dst[...] = (wide[slot, k] * scale).astype(BF16)

    def piece(source, q):
        return x_ref.at[pl.ds(pl.multiple_of(source * count + q * part, part), part), :]

    def token_first(up):
        src = pack.at[pl.ds(pl.multiple_of(t * part, part), part), :]
        where = (g, f + 1, t) if up else (g, f - 1, t)
        return remote(src, piece(f, t), ts.at[0 if up else 1, f], tr.at[f], where)

    def token_on(source, up):
        where = (g, f + 1, t) if up else (g, f - 1, t)
        here = piece(source, t)
        return remote(here, here, ts.at[0 if up else 1, source], tr.at[source], where)

    def each_token(d, act):
        for up in (True, False):
            source = f - d if up else f + d

            @pl.when((source >= 0) & (source < n))
            def _():
                act(source, up, (f + 1 < n) if up else (f > 0))

    def token_in(source):
        return remote(piece(source, t), piece(source, t), ts.at[0, 0], tr.at[source], (g, f, t))

    def token_over(source):
        here = piece(source, t)
        return remote(here, here, os.at[source], ov.at[source], (g, f, peers[2]))

    def token_from_over(source):
        here = piece(source, peers[2])
        return remote(here, here, os.at[source], ov.at[source], (g, f, peers[2]))

    def token_mate(source, j):
        here = piece(source, (t, peers[2])[j])
        return remote(here, here, ms.at[j, source], mr.at[j, source], (g, f, mate))

    def token_from_mate(source, j):
        here = piece(source, (mate, peers[3])[j])
        return remote(here, here, ms.at[j, source], mr.at[j, source], (g, f, mate))

    def token_own():
        return pltpu.make_async_copy(pack, x_ref.at[pl.ds(pl.multiple_of(f * count, count), count), :], own_sem.at[0])

    def send_tokens():
        for copy in small[1:]:
            copy.wait()
        values = tok[...].astype(F32)
        mean_square = jnp.mean(values * values, axis=-1, keepdims=True)
        pack[:, :depth] = (values * lax.rsqrt(mean_square + 1e-06)).astype(BF16)
        diff = logit_v[0:1, :] - logit_v[1:2, :]
        first_w = 1.0 / (1.0 + jnp.exp(-diff))
        second_w = 1.0 / (1.0 + jnp.exp(diff))
        eye = lax.broadcasted_iota(jnp.int32, (count, count), 0) == lax.broadcasted_iota(jnp.int32, (count, count), 1)
        lane = lax.broadcasted_iota(jnp.int32, (count, LANES), 1)
        table = jnp.zeros((count, LANES), F32)
        for e in range(n):
            line = first_w * (route_v[0:1, :] == e).astype(F32) + second_w * (route_v[1:2, :] == e).astype(F32)
            column = jnp.sum(jnp.where(eye, jnp.broadcast_to(line, (count, count)), 0.0), axis=1, keepdims=True)
            table = jnp.where(lane == e, jnp.broadcast_to(column, (count, LANES)), table)
        pack[:, depth:] = table.astype(BF16)
        token_own().start()

        @pl.when(f < n - 1)
        def _():
            token_first(True).start()

        @pl.when(f > 0)
        def _():
            token_first(False).start()

    def share_tokens(d):
        def act(source, up, more):
            token_in(source).wait_recv()

            @pl.when(more)
            def _():
                token_on(source, up).start()

            token_over(source).start()
            token_mate(source, 0).start()

        each_token(d, act)

    def pair_tokens():
        for d in range(1, n):
            source = lax.rem(f + d, n)
            token_from_over(source).wait_recv()
            token_mate(source, 1).start()

    def produce(i):
        for k in order:
            load(i, k, own_row).wait()
            fold(i % LOADS, k, own_row(i % CHUNKS), stage.at[k, i])
            if i + LOADS < items:
                load(i + LOADS, k, own_row).start()

            @pl.when(home)
            def _():
                if k == 0:
                    own_home(i).start()
                else:
                    first_home(k, i).start()

            if k >= 2:
                @pl.when(jnp.logical_not(home))
                def _():
                    first(k, i).start()

    def own(i, where):
        @pl.when(where)
        def _():
            direct(0, i).start()
            direct(1, i).start()

    def relay_home(i):
        for k in (2, 3):
            @pl.when(peers[k] == f)
            def _():
                first_home(k, i).wait_recv()
                across(f, i).start()

    def relay_near(i):
        for k in (2, 3):
            @pl.when(peers[k] == near)
            def _():
                first(k, i).wait_recv()
                layer(k, i).start()

    def relay_far(i, where):
        for k in (2, 3):
            @pl.when(where & (peers[k] != f) & (peers[k] != near))
            def _():
                first(k, i).wait_recv()
                layer(k, i).start()

    def turn(source, i):
        layer_in(source, i).wait_recv()
        across(source, i).start()

    def down_step(c):
        for k in order:
            load_d(k, c).wait()
            stage_d[k, c] = wide_d[c % DOWN_LOADS, k].astype(BF16)
            if c + DOWN_LOADS < DOWN_CHUNKS:
                load_d(k, c + DOWN_LOADS).start()
            down(k, c).start()

    def start_extra(i):
        @pl.when(home)
        def _():
            if i == 0:
                for j in range(min(LOADS, items)):
                    for k in (0, 1):
                        load(j, k, other_row).start()
            for k in (0, 1):
                load(i, k, other_row).wait()
                fold(i % LOADS, k, other_row(i % CHUNKS), extra.at[k, i])
                if i + LOADS < items:
                    load(i + LOADS, k, other_row).start()
                (extra_home if k == 0 else extra_mate)(i).start()

    outer = (f == 0) | (f == n - 1)
    inner = jnp.logical_not(outer)
    own_far = (t != near) & jnp.logical_not(home)
    send_tokens()
    for c in range(DOWN_LOADS):
        for k in order:
            load_d(k, c).start()
    sent = dict.fromkeys(("item", "inner own", "inner relay", "outer own", "outer relay", "near", "in", "out", "down", "extra"), 0)

    def start_item(i):
        produce(i)
        own(i, t == near)

    def up_to(name, limit, act):
        while sent[name] < min(limit, items):
            act(sent[name])
            sent[name] += 1

    sent["down"] = items - DOWN_CHUNKS
    s = 0
    while min(sent.values()) < items:
        paced = int(s * SEND_RATE)
        up_to("item", s + AHEAD, start_item)
        made = sent["item"]
        up_to("inner own", min(made, INNER_LEAD + paced), lambda i: own(i, own_far & inner))
        up_to("outer own", min(made, OUTER_LEAD + paced), lambda i: own(i, own_far & outer))
        if s < items:
            relay_home(s)
            relay_near(s)
        up_to("inner relay", min(s + 1, INNER_LEAD + paced), lambda i: relay_far(i, inner))
        up_to("outer relay", min(s + 1, OUTER_LEAD + paced), lambda i: relay_far(i, outer))
        if s % 2 == 0 and s // 2 + 1 < n:
            share_tokens(s // 2 + 1)
        if s == items + 1:
            pair_tokens()
        if s - items in DOWN_STEPS:
            down_step(DOWN_STEPS.index(s - items))
            sent["down"] += 1
        up_to("near", s + 1 - NEAR_LAG, lambda i: turn(near, i))
        up_to("in", int((s + 1 - IN_LAG) * FAR_RATE), lambda i: turn(far[0], i))
        up_to("out", int((s + 1 - OUT_LAG) * FAR_RATE), lambda i: turn(far[1], i))
        if made == items:
            up_to("extra", sent["extra"] + 1, start_extra)
        s += 1

    def finish(i):
        @pl.when(home)
        def _():
            own_home(i).wait()
            extra_home(i).wait()
            extra_mate(i).wait_send()
            first_home(1, i).wait_send()

        @pl.when(jnp.logical_not(home))
        def _():
            direct(0, i).wait_send()
            direct(1, i).wait_send()

        @pl.when(f == mate)
        def _():
            first_home(1, i).wait_recv()
            extra_mate(i).wait_recv()

        for k in (2, 3):
            first(k, i).wait_send()

            @pl.when(peers[k] != f)
            def _():
                layer(k, i).wait_send()

            @pl.when(peers[k] == f)
            def _():
                across(f, i).wait()

        for source in (near, *far):
            across(source, i).wait()

    for i in range(items):
        finish(i)

    def finish_d(c, _):
        for k in range(n):
            down(k, c).wait()
        return 0

    lax.fori_loop(0, DOWN_CHUNKS, finish_d, 0)
    token_own().wait()

    @pl.when(f < n - 1)
    def _():
        token_first(True).wait_send()

    @pl.when(f > 0)
    def _():
        token_first(False).wait_send()

    def sent_on(source, up, more):
        @pl.when(more)
        def _():
            token_on(source, up).wait_send()

    for d in range(1, n):
        each_token(d, sent_on)
    for d in range(1, n):
        source = lax.rem(f + d, n)
        token_over(source).wait_send()
        for j in range(2):
            token_mate(source, j).wait_send()
            token_from_mate(source, j).wait_recv()


def move(groups, n, tokens, routes, route_logits, gain, w_gate, w_up, w_down):
    experts, rows, cols = w_gate.shape
    hidden, width = w_down.shape[1:]
    count, depth = tokens.shape
    ch = rows // groups // CHUNKS
    dh = hidden // DOWN_CHUNKS
    items = 2 * CHUNKS
    dma = pltpu.SemaphoreType.DMA
    hbm = pl.BlockSpec(memory_space=pl.ANY)
    return pl.pallas_call(
        functools.partial(move_kernel, groups, n),
        out_shape=(
            pltpu.VMEM((count * n, depth + LANES), BF16),
            pltpu.VMEM((rows * n, cols), BF16),
            pltpu.VMEM((rows * n, cols), BF16),
            pltpu.VMEM((hidden, width * n), BF16),
        ),
        in_specs=[hbm] * 7,
        out_specs=(pl.BlockSpec(memory_space=pltpu.VMEM),) * 4,
        scratch_shapes=[
            pltpu.VMEM((LOADS, n, ch, cols), F32),
            pltpu.VMEM((DOWN_LOADS, n, dh, width), F32),
            pltpu.VMEM((n, items, ch, cols), BF16),
            pltpu.VMEM((2, items, ch, cols), BF16),
            pltpu.VMEM((2, items, ch, cols), BF16),
            pltpu.VMEM((n, DOWN_CHUNKS, dh, width), BF16),
            pltpu.VMEM((count, depth), BF16),
            pltpu.VMEM((count, depth + LANES), BF16),
            pltpu.VMEM((2, count), jnp.int32),
            pltpu.VMEM((2, count), F32),
            pltpu.VMEM((1, rows), F32),
            pltpu.VMEM((rows, LANES), F32),
            dma((LOADS, n)),
            dma((DOWN_LOADS, n)),
            dma((4,)),
            dma((n, items)),
            dma((n, items)),
            dma((2, items)),
            dma((items,)),
            dma((n, items)),
            dma((n, items)),
            dma((n, items)),
            dma((n, items)),
            dma((n, DOWN_CHUNKS)),
            dma((n, DOWN_CHUNKS)),
            dma((2, n)),
            dma((n,)),
            dma((n,)),
            dma((n,)),
            dma((2, n)),
            dma((2, n)),
            dma((1,)),
        ],
        name="move_weights",
        compiler_params=pltpu.CompilerParams(
            collective_id=0, has_side_effects=True, vmem_limit_bytes=40 << 20
        ),
    )(tokens, routes.T, route_logits.T, gain.reshape(1, rows), w_gate, w_up, w_down)


def mix_kernel(tile, x_ref, gate_ref, up_ref, down_ref, gate_out, up_out, down_out, term_ref, total, out_sem):
    copies = [
        pltpu.make_async_copy(src, dst, out_sem.at[i])
        for i, (src, dst) in enumerate(((gate_ref, gate_out), (up_ref, up_out), (down_ref, down_out)))
    ]
    for copy in copies:
        copy.start()
    depth = gate_ref.shape[0]
    lane = lax.broadcasted_iota(jnp.int32, (x_ref.shape[0], LANES), 1)
    table = jnp.where(lane == lax.axis_index("tp"), x_ref[:, depth:].astype(F32), 0.0)
    scale = jnp.sum(table, axis=1, keepdims=True)
    total[...] = jnp.zeros_like(total)

    def trip(j, _):
        cols = pl.ds(pl.multiple_of(j * tile, tile), tile)
        x = x_ref[:, :depth]
        gate_act = jnp.dot(x, gate_ref[:, cols], preferred_element_type=F32)
        up_act = jnp.dot(x, up_ref[:, cols], preferred_element_type=F32)
        hidden = (gate_act / (1.0 + jnp.exp(-gate_act)) * up_act * scale).astype(BF16)
        total[...] += jnp.dot(hidden, down_ref[cols, :], preferred_element_type=F32)
        return 0

    lax.fori_loop(0, gate_ref.shape[1] // tile, trip, 0)
    term_ref[...] = total[...].astype(BF16)
    for copy in copies:
        copy.wait()


def mix(packed, gate, up, down):
    count = packed.shape[0]
    cols = gate.shape[1]
    wide = down.shape[1]
    tile = next(w for w in (256, 128) if cols % w == 0)
    vmem = pl.BlockSpec(memory_space=pltpu.VMEM)
    hbm = pl.BlockSpec(memory_space=pl.ANY)
    return pl.pallas_call(
        functools.partial(mix_kernel, tile),
        out_shape=(
            jax.ShapeDtypeStruct(gate.shape, BF16),
            jax.ShapeDtypeStruct(up.shape, BF16),
            jax.ShapeDtypeStruct(down.shape, BF16),
            pltpu.VMEM((count, wide), BF16),
        ),
        in_specs=[vmem] * 4,
        out_specs=(hbm, hbm, hbm, vmem),
        scratch_shapes=[pltpu.VMEM((count, wide), F32), pltpu.SemaphoreType.DMA((3,))],
        name="mix_tokens",
        compiler_params=pltpu.CompilerParams(vmem_limit_bytes=12 << 20),
    )(packed, gate, up, down)


def sum_kernel(n, term_ref, out_ref, near, near_in, far, far_in, last, last_in, s1, r1, s2, r2, s3, r3):
    g, f, t = lax.axis_index("grp"), lax.axis_index("fs"), lax.axis_index("tp")
    mesh_id = pl.DeviceIdType.MESH
    width = out_ref.shape[1]
    count = out_ref.shape[0]
    mate = t + 1 - 2 * lax.rem(t, 2)
    over = lax.rem(t + 2, n)
    mate_over = lax.rem(mate + 2, n)

    barrier = pltpu.get_barrier_semaphore()
    for e in (mate, over):
        pl.semaphore_signal(barrier, inc=1, device_id=(g, f, e), device_id_type=mesh_id)
    for d in range(1, n):
        pl.semaphore_signal(barrier, inc=1, device_id=(g, lax.rem(f + d, n), t), device_id_type=mesh_id)
    pl.semaphore_wait(barrier, n + 1)

    def block(layer, column):
        return term_ref.at[pl.ds(pl.multiple_of(layer * count, count), count), pl.ds(pl.multiple_of(column * width, width), width)]

    def remote(src, dst, ssem, rsem, where):
        return pltpu.make_async_remote_copy(
            src_ref=src, dst_ref=dst, send_sem=ssem, recv_sem=rsem, device_id=where, device_id_type=mesh_id
        )

    layers = [lax.rem(f + d, n) for d in (2, 1, 3, 0)]

    def to_mate(i, h):
        column = mate_over if h == 0 else mate
        return remote(block(layers[i], column), near_in.at[h, i], s1.at[h, i], r1.at[h, i], (g, f, mate))

    def to_over(i):
        return remote(far.at[i], far_in.at[i], s2.at[i], r2.at[i], (g, f, over))

    def to_layer(i):
        return remote(last.at[i], last_in.at[f], s3.at[i], r3.at[f], (g, layers[i], t))

    def from_layer(layer):
        return remote(last.at[0], last_in.at[layer], s3.at[0], r3.at[layer], (g, layer, t))

    for i in range(n):
        for h in range(2):
            to_mate(i, h).start()
    for i in range(n):
        to_mate(i, 0).wait_recv()
        far[i] = (block(layers[i], over)[...].astype(F32) + near_in[0, i].astype(F32)).astype(BF16)
        to_mate(i, 1).wait_recv()
        near[i] = block(layers[i], t)[...].astype(F32) + near_in[1, i].astype(F32)
        to_over(i).start()
    for i in range(n):
        to_over(i).wait_recv()
        near[i] = near[i] + far_in[i].astype(F32)
        if i < n - 1:
            last[i] = near[i].astype(BF16)
            to_layer(i).start()
    total = near[n - 1]
    for d in range(1, n):
        layer = lax.rem(f + d, n)
        from_layer(layer).wait_recv()
        total = total + last_in[layer].astype(F32)
    out_ref[...] = total.astype(BF16)
    for i in range(n):
        for h in range(2):
            to_mate(i, h).wait_send()
        to_over(i).wait_send()
        if i < n - 1:
            to_layer(i).wait_send()


def sum_terms(n, term):
    count, width = term.shape[0] // n, term.shape[1] // n
    dma = pltpu.SemaphoreType.DMA
    vmem = pl.BlockSpec(memory_space=pltpu.VMEM)
    piece = (count, width)
    return pl.pallas_call(
        functools.partial(sum_kernel, n),
        out_shape=jax.ShapeDtypeStruct(piece, BF16),
        in_specs=[vmem],
        out_specs=vmem,
        scratch_shapes=[
            pltpu.VMEM((n, *piece), F32),
            pltpu.VMEM((2, n, *piece), BF16),
            pltpu.VMEM((n, *piece), BF16),
            pltpu.VMEM((n, *piece), BF16),
            pltpu.VMEM((n, *piece), BF16),
            pltpu.VMEM((n, *piece), BF16),
            dma((2, n)), dma((2, n)), dma((n,)), dma((n,)), dma((n,)), dma((n,)),
        ],
        name="sum_terms",
        compiler_params=pltpu.CompilerParams(collective_id=1, has_side_effects=True, vmem_limit_bytes=8 << 20),
    )(term)


def fits(mesh, tokens, w_gate, w_down):
    groups, n, tp = mesh.shape["grp"], mesh.shape["fs"], mesh.shape["tp"]
    rows, cols = w_gate.shape[1:]
    hidden, width = w_down.shape[1:]
    return (
        groups == 2 and n == 4 and tp == 4 and w_gate.shape[0] == tp
        and cols == hidden and cols % 128 == 0 and width % 128 == 0 and tokens.shape[0] % (16 * n) == 0
        and rows % (groups * CHUNKS * 16) == 0 and hidden % (DOWN_CHUNKS * 16) == 0
        and tokens.shape[0] * n <= 512 and rows % LANES == 0 and rows * n == tokens.shape[1]
    )


def body(mesh, tokens, routes, route_logits, gain, w_gate, w_up, w_down):
    n, depth = mesh.shape["fs"], tokens.shape[1]
    if fits(mesh, tokens, w_gate, w_down):
        packed, gate, up, down = move(mesh.shape["grp"], n, tokens, routes, route_logits, gain, w_gate, w_up, w_down)
        gate, up, down, term = mix(packed, gate, up, down)
        return gate[None], up[None], down[None], sum_terms(n, term)
    values = tokens.astype(F32)
    mean_square = jnp.mean(values * values, axis=-1, keepdims=True)
    normed = (values * lax.rsqrt(mean_square + 1e-06)).astype(BF16)
    expert_id = lax.axis_index("tp")
    first = jax.nn.sigmoid(route_logits[:, 0] - route_logits[:, 1])
    second = jax.nn.sigmoid(route_logits[:, 1] - route_logits[:, 0])
    weight_col = first * (routes[:, 0] == expert_id).astype(F32)
    weight_col = (weight_col + second * (routes[:, 1] == expert_id).astype(F32)).astype(BF16)
    packed = jnp.concatenate([normed, jnp.broadcast_to(weight_col[:, None], (normed.shape[0], 128))], axis=1)
    packed = lax.all_gather(packed, "fs", axis=0, tiled=True)
    gate = (w_gate * gain[None, :, None]).astype(BF16)
    up = (w_up * gain[None, :, None]).astype(BF16)
    spread = functools.partial(lax.all_to_all, axis_name="tp", split_axis=0, concat_axis=2, tiled=True)
    gate, up, down = spread(gate), spread(up), spread(w_down.astype(BF16))
    stack = functools.partial(lax.all_to_all, axis_name="fs", split_axis=2, concat_axis=1, tiled=True)
    gate, up = stack(gate), stack(up)
    rows, weight = packed[:, :depth], packed[:, depth : depth + 1]
    gate_act = jnp.dot(rows, gate[0], preferred_element_type=F32)
    up_act = jnp.dot(rows, up[0], preferred_element_type=F32)
    hidden = (jax.nn.silu(gate_act) * up_act * weight.astype(F32)).astype(BF16)
    term = jnp.dot(hidden, down[0], preferred_element_type=F32)
    by_feature = lax.psum_scatter(term, "tp", scatter_dimension=1, tiled=True)
    mixed = lax.psum_scatter(by_feature, "fs", scatter_dimension=0, tiled=True)
    return gate, up, down, mixed.astype(BF16)


def solution(mesh):
    return jax.shard_map(
        functools.partial(body, mesh),
        mesh=mesh,
        in_specs=(
            P(("grp", "fs"), None),
            P(("grp", "fs"), None),
            P(("grp", "fs"), None),
            P("fs"),
            P(None, "fs", "tp"),
            P(None, "fs", "tp"),
            P(None, "fs", "tp"),
        ),
        out_specs=(
            P(("grp", "tp"), None, "fs"),
            P(("grp", "tp"), None, "fs"),
            P(("grp", "tp"), "fs", None),
            P(("grp", "fs"), "tp"),
        ),
        check_vma=False,
    )
```
